32 devices in a mesh: ep: 16 (over z, y, x), tp: 2 (over core).
Axes of the slice: x: 2, y: 2, z: 4, core: 2. Of those that a mesh axis runs over, the one named last changes fastest.
Arguments:
- tokens_in: bfloat16 [512, 2048], P('ep'), may hold values from -6 to 6
- state_in: float32 [512, 8, 64, 64], P('ep', 'tp'), may hold values from -4 to 4
- norm_mix: bfloat16 [2048], replicated, may hold values from 0.099609375 to 1.8984375
- w_recept: bfloat16 [2048, 512], P(None, 'tp'), may hold values from -0.125 to 0.125
- w_key: bfloat16 [2048, 512], P(None, 'tp'), may hold values from -0.125 to 0.125
- w_value: bfloat16 [2048, 512], P(None, 'tp'), may hold values from -0.125 to 0.125
- decay_down: bfloat16 [2048, 64], replicated, may hold values from -0.125 to 0.125
- decay_up: bfloat16 [64, 512], P(None, 'tp'), may hold values from -0.75 to 0.75
- decay_base: float32 [512], P('tp'), may hold values from -4 to 2
- iclr_down: bfloat16 [2048, 64], replicated, may hold values from -0.125 to 0.125
- iclr_up: bfloat16 [64, 512], P(None, 'tp'), may hold values from -0.75 to 0.75
- iclr_base: float32 [512], P('tp'), may hold values from -4 to 4
- key_scale: bfloat16 [512], P('tp'), may hold values from 0.099609375 to 1.8984375
- key_mix: bfloat16 [512], P('tp'), may hold values from 0.099609375 to 1.8984375
- w_out: bfloat16 [512, 2048], P('tp'), may hold values from -0.046875 to 0.046875
- norm_moe: bfloat16 [2048], replicated, may hold values from 0.099609375 to 1.8984375
- router_group: bfloat16 [2048, 2], replicated, may hold values from -0.125 to 0.125
- router_expert: bfloat16 [2048, 16], replicated, may hold values from -0.125 to 0.125
- routes: int32 [512, 4], P('ep'), may hold values from 0 to 15, as said below
- expert_gate: bfloat16 [16, 2048, 256], P('ep', None, 'tp'), may hold values from -0.125 to 0.125
- expert_up: bfloat16 [16, 2048, 256], P('ep', None, 'tp'), may hold values from -0.125 to 0.125
- expert_down: bfloat16 [16, 256, 2048], P('ep', 'tp'), may hold values from -1.5 to 1.5
Outputs:
- layer_out: bfloat16 [512, 2048], P('ep', 'tp')
- state_out: float32 [512, 8, 64, 64], P('ep', 'tp')
The draws below stay inside these ranges and needn't reach their ends.
Inputs may be any that keep to these rules, and one draw needn't show every extreme that they name: `routes`: each row names 4 different experts of one group (the same value of id // 8). Among the rows of one device no expert is named by more than 16 rows, and in every draw one expert is named by exactly 16 rows of every device.
All inputs are finite; a program needn't handle non-finite values.
Results may differ from the reference program's by a relative error of at most 0.018.
Values may be sent and summed in bfloat16 or wider, within the bound.
A program may use at most 64 MiB of HBM per device.

```python
import jax
import jax.numpy as jnp
from jax import lax

D = 2048
HEADS = 8
HEAD = 64
RANK = 64
FE = 256
GROUP_EXPERTS = 8
TOPK = 4
SEQ_DEV = 32
WIDTH = 512
TOKENS = 512
EXPERTS = 16
GROUPS = 2
CAP = 16
N_EP = 16
N_TP = 2


def draw_routes(key, part):
    base = jax.random.fold_in(key, 7)
    keys = jax.random.split(base, 7)
    blocks = TOKENS // SEQ_DEV
    total_rows = blocks * SEQ_DEV
    hot_group = jax.random.randint(keys[0], (), 0, GROUPS)
    hot_inner = jax.random.randint(keys[1], (), 0, GROUP_EXPERTS)
    order = jax.vmap(lambda sub: jax.random.permutation(sub, SEQ_DEV))(jax.random.split(keys[2], blocks))
    band = order // CAP
    others = jax.vmap(lambda sub: jax.random.permutation(sub, max(GROUPS - 1, 1)))(jax.random.split(keys[3], blocks))
    chosen = jnp.take_along_axis(others, jnp.maximum(band - 1, 0), axis=1)
    group_ids = jnp.where(band == 0, hot_group, (hot_group + 1 + chosen) % GROUPS).reshape(total_rows, 1)
    free_pick = jax.vmap(lambda sub: jax.random.permutation(sub, GROUP_EXPERTS))(jax.random.split(keys[4], total_rows))[:, :TOPK]
    rest = jax.vmap(lambda sub: jax.random.permutation(sub, GROUP_EXPERTS - 1))(jax.random.split(keys[5], total_rows))[:, :TOPK - 1]
    forced = jnp.concatenate([jnp.zeros((total_rows, 1), jnp.int32) + hot_inner, (hot_inner + 1 + rest) % GROUP_EXPERTS], axis=1)
    inner = jnp.where(band.reshape(total_rows, 1) == 0, forced, free_pick)
    column_order = jax.vmap(lambda sub: jax.random.permutation(sub, TOPK))(jax.random.split(keys[6], total_rows))
    inner = jnp.take_along_axis(inner, column_order, axis=1)
    return (group_ids * GROUP_EXPERTS + inner).astype(jnp.int32)


def steps_of(rng, extent, pieces, least, high):
    gain = 1.0
    for dim, parts in pieces:
        draws = jax.random.uniform(jax.random.fold_in(jax.random.fold_in(rng, 6), dim), (parts,), jnp.float32, least / len(pieces), high / len(pieces))
        gain = gain * jnp.repeat(jnp.exp(draws), extent[dim] // parts).reshape((-1,) + (1,) * (len(extent) - 1 - dim))
    return gain


def centred(own_key, shape, scale, reach, shards=(), held_as=jnp.bfloat16):
    values = jax.random.normal(own_key, shape, jnp.float32) * scale
    if len(shards) > 0:
        values = steps_of(own_key, shape, shards, -0.22, 0.18) * values
    return jnp.clip(values, min=-reach, max=reach).astype(held_as)


def setup_inputs(seed: int = 0) -> dict:
    streams_of = jax.random.split(jax.random.key(seed), 23)
    return {
        "tokens_in": centred(streams_of[0], (TOKENS, D), 1.0, 6.0, ((0, 16),)),
        "state_in": centred(streams_of[1], (TOKENS, HEADS, HEAD, HEAD), 0.5, 4.0, ((0, 16), (1, 2)), jnp.float32),
        "norm_mix": jnp.clip(1.0 + 0.18 * jax.random.normal(streams_of[2], (D,), jnp.float32), 0.099609375, 1.8984375).astype(jnp.bfloat16),
        "w_recept": centred(streams_of[3], (D, WIDTH), D ** -0.5, 0.125, ((1, 2),)),
        "w_key": centred(streams_of[4], (D, WIDTH), D ** -0.5, 0.125, ((1, 2),)),
        "w_value": centred(streams_of[5], (D, WIDTH), D ** -0.5, 0.125, ((1, 2),)),
        "decay_down": centred(streams_of[6], (D, RANK), D ** -0.5, 0.125),
        "decay_up": centred(streams_of[7], (RANK, WIDTH), RANK ** -0.5, 0.75, ((1, 2),)),
        "decay_base": jnp.clip(-4.0 + 6.0 * jax.random.uniform(streams_of[8], (WIDTH,), jnp.float32) ** steps_of(streams_of[8], (WIDTH,), ((0, 2),), -0.2, 0.2), -4.0, 2.0),
        "iclr_down": centred(streams_of[9], (D, RANK), D ** -0.5, 0.125),
        "iclr_up": centred(streams_of[10], (RANK, WIDTH), RANK ** -0.5, 0.75, ((1, 2),)),
        "iclr_base": centred(streams_of[11], (WIDTH,), 1.0, 4.0, ((0, 2),), jnp.float32),
        "key_scale": jnp.clip(1.0 + 0.18 * jax.random.normal(streams_of[12], (WIDTH,), jnp.float32), 0.099609375, 1.8984375).astype(jnp.bfloat16),
        "key_mix": jnp.clip(1.0 + 0.18 * jax.random.normal(streams_of[13], (WIDTH,), jnp.float32), 0.099609375, 1.8984375).astype(jnp.bfloat16),
        "w_out": centred(streams_of[14], (WIDTH, D), (32 * WIDTH) ** -0.5, 0.046875, ((0, 2),)),
        "norm_moe": jnp.clip(1.0 + 0.18 * jax.random.normal(streams_of[15], (D,), jnp.float32), 0.099609375, 1.8984375).astype(jnp.bfloat16),
        "router_group": centred(streams_of[16], (D, GROUPS), D ** -0.5, 0.125),
        "router_expert": centred(streams_of[17], (D, EXPERTS), D ** -0.5, 0.125),
        "routes": draw_routes(jax.random.fold_in(streams_of[22], 71), 0),
        "expert_gate": centred(streams_of[19], (EXPERTS, D, FE), D ** -0.5, 0.125, ((0, 16), (2, 2))),
        "expert_up": centred(streams_of[20], (EXPERTS, D, FE), D ** -0.5, 0.125, ((0, 16), (2, 2))),
        "expert_down": centred(streams_of[21], (EXPERTS, FE, D), (FE // 16) ** -0.5, 1.5, ((0, 16), (1, 2))),
    }


def rms_scale(values, weights):
    values32 = values.astype(jnp.float32)
    factor = lax.rsqrt(lax.optimization_barrier(jnp.mean(values32 * values32, axis=-1, keepdims=True)) + 1e-06)
    return (values32 * factor * weights.astype(jnp.float32)).astype(jnp.bfloat16)

def split_heads(values):
    return values.astype(jnp.float32).reshape(values.shape[0], HEADS, HEAD)

def expert_rows(moe_rows, gate_weight, up_weight, down_weight):
    gate_part = jnp.dot(moe_rows, gate_weight, preferred_element_type=jnp.float32)
    up_part = jnp.dot(moe_rows, up_weight, preferred_element_type=jnp.float32)
    hidden = (jax.nn.silu(gate_part) * up_part).astype(jnp.bfloat16)
    block = FE // N_TP
    total = jnp.zeros((moe_rows.shape[0], D), jnp.float32)
    for index in range(N_TP):
        partial_value = jnp.dot(hidden[:, index * block:(index + 1) * block], down_weight[index * block:(index + 1) * block], preferred_element_type=jnp.float32).astype(jnp.bfloat16)
        partial_value = lax.optimization_barrier(partial_value)
        total = total + partial_value.astype(jnp.float32)
    return total.astype(jnp.bfloat16)

def reference(tokens_in, state_in, norm_mix, w_recept, w_key, w_value, decay_down, decay_up, decay_base, iclr_down, iclr_up, iclr_base, key_scale, key_mix, w_out, norm_moe, router_group, router_expert, routes, expert_gate, expert_up, expert_down):
    f32 = jnp.float32
    bf16 = jnp.bfloat16
    normed = rms_scale(tokens_in, norm_mix)
    recept = jnp.dot(normed, w_recept, preferred_element_type=f32).astype(bf16)
    key_rows = jnp.dot(normed, w_key, preferred_element_type=f32).astype(bf16)
    value_rows = jnp.dot(normed, w_value, preferred_element_type=f32).astype(bf16)
    decay_low = jnp.tanh(jnp.dot(normed, decay_down, preferred_element_type=f32)).astype(bf16)
    iclr_low = jnp.dot(normed, iclr_down, preferred_element_type=f32).astype(bf16)
    log_rate = -jax.nn.softplus(-(decay_base.astype(f32) + jnp.dot(decay_low, decay_up, preferred_element_type=f32))) - 0.5
    decays = jnp.exp(-jnp.exp(log_rate))
    learn_rate = jax.nn.sigmoid(iclr_base.astype(f32) + jnp.dot(iclr_low, iclr_up, preferred_element_type=f32))
    recept_heads = split_heads(recept)
    key_heads = split_heads(key_rows)
    value_heads = split_heads(value_rows)
    rate_heads = split_heads(learn_rate)
    decay_heads = split_heads(decays)
    scaled = key_heads * key_scale.astype(f32).reshape(HEADS, HEAD)
    unit_key = scaled * lax.rsqrt(lax.optimization_barrier(jnp.sum(scaled * scaled, axis=-1, keepdims=True)) + 1e-06)
    key_mod = key_heads * (1.0 + (rate_heads - 1.0) * key_mix.astype(f32).reshape(HEADS, HEAD))
    removed = jnp.einsum('shvk,shk->shv', state_in, unit_key)
    state_out = state_in * decay_heads[:, :, None, :] - removed[..., None] * (unit_key * rate_heads)[:, :, None, :] + value_heads[..., None] * key_mod[:, :, None, :]
    mixed = jnp.einsum('shvk,shk->shv', state_out, recept_heads).reshape(TOKENS, WIDTH).astype(bf16)
    mixer_out = jnp.dot(mixed, w_out, preferred_element_type=f32).astype(bf16)
    x_mid = (tokens_in.astype(f32) + mixer_out.astype(f32)).astype(bf16)
    moe_in = rms_scale(x_mid, norm_moe)
    group_id = routes[:, 0] // GROUP_EXPERTS
    group_logit = jnp.dot(moe_in, router_group, preferred_element_type=f32)
    group_hit = group_id[:, None] == jnp.arange(GROUPS, dtype=jnp.int32)[None, :]
    group_prob = jax.nn.sigmoid(lax.optimization_barrier(jnp.sum(jnp.where(group_hit, group_logit, 0.0), axis=1)))
    expert_logit = jnp.dot(moe_in, router_expert, preferred_element_type=f32)
    expert_hit = routes[:, :, None] == jnp.arange(EXPERTS, dtype=jnp.int32)[None, None, :]
    scores = jax.nn.sigmoid(lax.optimization_barrier(jnp.sum(jnp.where(expert_hit, expert_logit[:, None, :], 0.0), axis=2)))
    route_weight = group_prob[:, None] * scores / lax.optimization_barrier(jnp.sum(scores, axis=1, keepdims=True))
    limit = N_EP * CAP

    def visit(total, inputs):
        gate_weight, up_weight, down_weight, expert_index = inputs
        used = jnp.any(routes == expert_index, axis=1)
        found = jnp.nonzero(used, size=limit, fill_value=TOKENS)[0].astype(jnp.int32)
        valid = (found < TOKENS).astype(f32)
        safe = jnp.minimum(found, TOKENS - 1).astype(jnp.int32)
        results = expert_rows(moe_in[safe], gate_weight, up_weight, down_weight)
        weight = lax.optimization_barrier(jnp.sum(jnp.where(routes[safe] == expert_index, route_weight[safe], 0.0), axis=1)) * valid
        return (total.at[safe].add(weight[:, None] * results.astype(f32)), None)
    total, unused = lax.scan(visit, jnp.zeros((TOKENS, D), f32), (expert_gate, expert_up, expert_down, jnp.arange(EXPERTS, dtype=jnp.int32)))
    layer_out = (x_mid.astype(f32) + total).astype(bf16)
    return (layer_out, state_out)
```

```python
import functools

import jax
import jax.numpy as jnp
from jax import lax
from jax.experimental import pallas as pl
from jax.experimental.pallas import tpu as pltpu
from jax.sharding import PartitionSpec as P


def mixer_kernel(
    tokens_ref, norm_ref, w_recept_hbm, w_key_hbm, w_value_hbm, decay_down_ref, decay_up_ref, decay_base_ref,
    iclr_down_ref, iclr_up_ref, iclr_base_ref, key_scale_ref, key_mix_ref, state_hbm,
    mixed_ref, state_out_hbm,
    weights, state_buf, out_buf, weight_sems, in_sems, out_sems,
):
    f32 = jnp.float32
    bf16 = jnp.bfloat16
    seq_count, width = tokens_ref.shape
    heads, head_size = state_hbm.shape[1], state_hbm.shape[3]
    channels = heads * head_size
    n_chunks = in_sems.shape[0]
    per_chunk = seq_count // n_chunks
    rows_dims = (((1,), (1,)), ((), ()))
    weight_loads = [
        pltpu.make_async_copy(source, weights.at[index], weight_sems.at[index])
        for index, source in enumerate((w_key_hbm, w_recept_hbm, w_value_hbm))
    ]
    for load in weight_loads:
        load.start()
    state_loads = []
    state_stores = []
    for index in range(n_chunks):
        span = pl.ds(index * per_chunk, per_chunk)
        state_loads.append(
            pltpu.make_async_copy(state_hbm.at[span], state_buf.at[span], in_sems.at[index])
        )
        state_stores.append(
            pltpu.make_async_copy(out_buf.at[span], state_out_hbm.at[span], out_sems.at[index])
        )
        state_loads[index].start()

    tokens = tokens_ref[...].astype(f32)
    factor = lax.rsqrt(jnp.mean(tokens * tokens, axis=1, keepdims=True) + 1e-06)
    normed = (tokens * factor * norm_ref[...].reshape(1, width).astype(f32)).astype(bf16)
    decay_low = jnp.tanh(
        lax.dot_general(normed, decay_down_ref[...], rows_dims, preferred_element_type=f32)
    ).astype(bf16)
    iclr_low = lax.dot_general(
        normed, iclr_down_ref[...], rows_dims, preferred_element_type=f32
    ).astype(bf16)
    decay_in = decay_base_ref[...].reshape(1, channels) + jnp.dot(
        decay_low, decay_up_ref[...], preferred_element_type=f32
    )
    decays = jnp.exp(-jnp.exp(jnp.float32(-0.5)) * jax.nn.sigmoid(decay_in))
    rate = jax.nn.sigmoid(
        iclr_base_ref[...].reshape(1, channels)
        + jnp.dot(iclr_low, iclr_up_ref[...], preferred_element_type=f32)
    )

    def project(index):
        weight_loads[index].wait()
        rows = jnp.dot(normed, weights[index], preferred_element_type=f32)
        return rows.astype(bf16).astype(f32)

    key = project(0)
    scaled = key * key_scale_ref[...].reshape(1, channels).astype(f32)
    key_mod = key * (1.0 + (rate - 1.0) * key_mix_ref[...].reshape(1, channels).astype(f32))
    spans = [slice(head * head_size, (head + 1) * head_size) for head in range(heads)]
    units = []
    for span in spans:
        part = scaled[:, span]
        units.append(part * lax.rsqrt(jnp.sum(part * part, axis=1, keepdims=True) + 1e-06))
    recept = project(1)
    readers, writers, gains = [], [], []
    for head, span in enumerate(spans):
        unit, query = units[head], recept[:, span]
        drop = unit * rate[:, span]
        shift = jnp.sum(drop * query, axis=1, keepdims=True)
        gains.append(jnp.sum(key_mod[:, span] * query, axis=1, keepdims=True))
        reader = decays[:, span] * query - unit * shift
        readers.append(jnp.concatenate([unit, reader], axis=0).astype(bf16))
        writers.append(jnp.concatenate([-drop, key_mod[:, span]], axis=0).astype(bf16))
    value = project(2)
    value_t = jnp.concatenate([value, value], axis=0).T

    lanes = lax.broadcasted_iota(jnp.int32, (per_chunk, head_size, 2 * seq_count), 2)
    seqs = lax.broadcasted_iota(jnp.int32, (per_chunk, head_size, 2 * seq_count), 0)
    first = lanes < seq_count
    owner = jnp.where(first, lanes, lanes - seq_count)
    totals = [jnp.zeros((head_size, 2 * seq_count), f32) for _ in range(heads)]
    for index in range(n_chunks):
        rows = slice(index * per_chunk, (index + 1) * per_chunk)
        here = owner == seqs + index * per_chunk
        state_loads[index].wait()
        for head, span in enumerate(spans):
            state = state_buf[rows, head]
            flat = state.reshape(per_chunk * head_size, head_size).astype(bf16)
            read = lax.dot_general(flat, readers[head], rows_dims, preferred_element_type=f32)
            read = read.reshape(per_chunk, head_size, 2 * seq_count)
            totals[head] += jnp.sum(jnp.where(here, read, 0.0), axis=0)
            terms = jnp.where(here, jnp.where(first, read, value_t[span, :][None]), 0.0)
            terms = terms.reshape(per_chunk * head_size, 2 * seq_count).astype(bf16)
            change = jnp.dot(terms, writers[head], preferred_element_type=f32)
            out_buf[rows, head] = state * decays[rows, span][:, None, :] + change.reshape(
                per_chunk, head_size, head_size
            )
        state_stores[index].start()
    total = jnp.concatenate(totals, axis=0).T[seq_count:]
    for head, span in enumerate(spans):
        mixed_ref[:, span] = (total[:, span] + value[:, span] * gains[head]).astype(bf16)
    for store in state_stores:
        store.wait()


def moe_kernel(
    ep_count,
    block_rows,
    mixed_ref,
    w_out_hbm,
    tokens_ref,
    norm_ref,
    router_group_ref,
    router_expert_ref,
    routes_ref,
    gate_hbm,
    up_hbm,
    down_hbm,
    moe_ref,
    mid_ref,
    gate_ref,
    up_ref,
    down_ref,
    w_out_ref,
    part_buf,
    part_recv,
    mid_buf,
    norm_buf,
    send_buf,
    rows_buf,
    hidden_buf,
    term_send,
    term_own,
    term_recv,
    result_buf,
    back_buf,
    part_sems,
    out_send_sems,
    out_recv_sems,
    pair_send_sems,
    pair_recv_sems,
    term_send_sems,
    term_recv_sems,
    back_send_sems,
    back_recv_sems,
    load_sems,
):
    f32 = jnp.float32
    bf16 = jnp.bfloat16
    me = lax.axis_index("ep")
    core = lax.axis_index("tp")
    other = 1 - core
    seq_count, width = tokens_ref.shape
    half = width // 2
    cap = send_buf.shape[1]
    total_rows = ep_count * cap
    per_block = block_rows // cap
    n_blocks = total_rows // block_rows
    mesh_ids = pl.DeviceIdType.MESH

    def peer_at(step):
        return lax.rem(me + step, ep_count)

    def step_at(index):
        return 1 + lax.rem(index + ep_count // 2 - 1, ep_count - 1)

    barrier = pltpu.get_barrier_semaphore()
    pl.semaphore_signal(barrier, inc=1, device_id=(me, other), device_id_type=mesh_ids)

    def greet(step, carry):
        pl.semaphore_signal(
            barrier, inc=1, device_id=(peer_at(step), core), device_id_type=mesh_ids
        )
        return carry

    lax.fori_loop(1, ep_count, greet, 0)

    loads = [
        pltpu.make_async_copy(w_out_hbm, w_out_ref, load_sems.at[0]),
        pltpu.make_async_copy(gate_hbm.at[0], gate_ref, load_sems.at[1]),
        pltpu.make_async_copy(up_hbm.at[0], up_ref, load_sems.at[2]),
        pltpu.make_async_copy(down_hbm.at[0, :, pl.ds(0, half)], down_ref.at[0], load_sems.at[3]),
        pltpu.make_async_copy(down_hbm.at[0, :, pl.ds(half, half)], down_ref.at[1], load_sems.at[4]),
    ]
    for load in loads:
        load.start()

    n_groups = router_group_ref.shape[0]
    expert_ids = lax.broadcasted_iota(jnp.int32, (ep_count, seq_count), 0)
    uses = jnp.zeros((ep_count, seq_count), f32)
    for index in range(routes_ref.shape[0]):
        uses += jnp.where(routes_ref[index : index + 1, :] == expert_ids, 1.0, 0.0)
    group_ids = lax.broadcasted_iota(jnp.int32, (n_groups, seq_count), 0)
    group_hit = jnp.where(
        routes_ref[0:1, :] // (ep_count // n_groups) == group_ids, 1.0, 0.0
    )
    row_ids = lax.broadcasted_iota(jnp.int32, (seq_count, seq_count), 0)
    column_ids = lax.broadcasted_iota(jnp.int32, (seq_count, seq_count), 1)
    earlier = jnp.where(row_ids < column_ids, 1.0, 0.0).astype(bf16)
    position = jnp.dot(uses.astype(bf16), earlier, preferred_element_type=f32)
    slots = jnp.where(uses > 0.5, position, -1.0).astype(bf16)
    slot_rows = lax.broadcasted_iota(jnp.int32, (total_rows, ep_count), 0)
    slot_experts = lax.broadcasted_iota(jnp.int32, (total_rows, ep_count), 1)
    spread = jnp.where(slot_rows // cap == slot_experts, 1.0, 0.0).astype(bf16)
    slot_of_row = lax.broadcasted_iota(jnp.int32, (total_rows, seq_count), 0) % cap
    hits = jnp.dot(spread, slots, preferred_element_type=f32) == slot_of_row.astype(f32)
    chooser = jnp.where(hits, 1.0, 0.0)
    placement = chooser.astype(bf16)

    loads[0].wait()
    for index in range(2):
        columns = slice(index * half, (index + 1) * half)
        part_buf[index] = jnp.dot(
            mixed_ref[...], w_out_ref[:, columns], preferred_element_type=f32
        )
    pl.semaphore_wait(barrier, ep_count)

    def pair_copy(source, target, send_sem, recv_sem):
        return pltpu.make_async_remote_copy(
            src_ref=source,
            dst_ref=target,
            send_sem=send_sem,
            recv_sem=recv_sem,
            device_id=(me, other),
            device_id_type=mesh_ids,
        )

    part_copy = pair_copy(part_buf, part_recv, part_sems.at[0], part_sems.at[1])
    part_copy.start()
    part_copy.wait()

    squares = jnp.zeros((seq_count, 1), f32)
    for index in range(2):
        columns = slice(index * half, (index + 1) * half)
        mixer_out = (part_buf[index] + part_recv[index]).astype(bf16)
        mid = (tokens_ref[:, columns].astype(f32) + mixer_out.astype(f32)).astype(bf16)
        mid_buf[index] = mid
        mid32 = mid.astype(f32)
        squares = squares + jnp.sum(mid32 * mid32, axis=1, keepdims=True)
    factor = lax.rsqrt(squares / width + 1e-06)
    for index in range(2):
        columns = slice(index * half, (index + 1) * half)
        norm_buf[index] = (
            mid_buf[index].astype(f32) * factor * norm_ref[columns].reshape(1, half).astype(f32)
        ).astype(bf16)

    own_norm = norm_buf[core]
    for index in range(n_blocks):
        rows = jnp.dot(
            placement[index * block_rows : (index + 1) * block_rows, :],
            own_norm,
            preferred_element_type=f32,
        ).astype(bf16)
        send_buf[index * per_block : (index + 1) * per_block] = rows.reshape(per_block, cap, half)

    def out_copy(step):
        peer = peer_at(step)
        return pltpu.make_async_remote_copy(
            src_ref=send_buf.at[peer],
            dst_ref=rows_buf.at[core, me],
            send_sem=out_send_sems.at[step],
            recv_sem=out_recv_sems.at[step],
            device_id=(peer, core),
            device_id_type=mesh_ids,
        )

    def rows_copy(step):
        source = lax.rem(me + ep_count - step, ep_count)
        return pair_copy(
            rows_buf.at[core, source],
            rows_buf.at[core, source],
            pair_send_sems.at[step],
            pair_recv_sems.at[step],
        )

    def rows_arrival(step):
        source = lax.rem(me + ep_count - step, ep_count)
        return pair_copy(
            rows_buf.at[other, source],
            rows_buf.at[other, source],
            pair_send_sems.at[step],
            pair_recv_sems.at[step],
        )

    def start_out(index, carry):
        out_copy(step_at(index)).start()
        return carry

    lax.fori_loop(0, ep_count - 1, start_out, 0)
    rows_buf[core, me] = send_buf[me]
    rows_copy(0).start()

    rows_dims = (((1,), (1,)), ((), ()))
    group_logit = jnp.zeros(group_hit.shape, f32)
    expert_logit = jnp.zeros(uses.shape, f32)
    for index in range(2):
        columns = slice(index * half, (index + 1) * half)
        group_logit += lax.dot_general(
            router_group_ref[:, columns], norm_buf[index], rows_dims, preferred_element_type=f32
        )
        expert_logit += lax.dot_general(
            router_expert_ref[:, columns], norm_buf[index], rows_dims, preferred_element_type=f32
        )
    group_prob = jax.nn.sigmoid(jnp.sum(group_logit * group_hit, axis=0, keepdims=True))
    scores = jax.nn.sigmoid(expert_logit) * uses
    weights = group_prob * scores / jnp.sum(scores, axis=0, keepdims=True)
    weights_high = weights.astype(bf16)
    weights_low = (weights - weights_high.astype(f32)).astype(bf16)
    combine_high = (jnp.dot(spread, weights_high, preferred_element_type=f32) * chooser).T
    combine_low = (jnp.dot(spread, weights_low, preferred_element_type=f32) * chooser).T
    combine_high = combine_high.astype(bf16)
    combine_low = combine_low.astype(bf16)
    mid_ref[...] = mid_buf[core]

    def relay(index, carry):
        step = step_at(ep_count - 2 - index)
        out_copy(step).wait_recv()
        rows_copy(step).start()
        return carry

    lax.fori_loop(0, ep_count - 1, relay, 0)

    def arrive(step, carry):
        rows_arrival(step).wait_recv()
        return carry

    lax.fori_loop(0, ep_count, arrive, 0)

    for load in loads[1:]:
        load.wait()
    for index in range(n_blocks):
        experts = slice(index * per_block, (index + 1) * per_block)
        gate_part = jnp.zeros((block_rows, gate_ref.shape[1]), f32)
        up_part = jnp.zeros((block_rows, gate_ref.shape[1]), f32)
        for piece in range(2):
            columns = slice(piece * half, (piece + 1) * half)
            rows = rows_buf[piece, experts].reshape(block_rows, half)
            gate_part += jnp.dot(rows, gate_ref[columns, :], preferred_element_type=f32)
            up_part += jnp.dot(rows, up_ref[columns, :], preferred_element_type=f32)
        hidden = (gate_part / (1.0 + jnp.exp(-gate_part)) * up_part).astype(bf16)
        hidden_buf[experts] = hidden.reshape(per_block, cap, gate_ref.shape[1])

    n_parts = term_send.shape[0]
    per_part = ep_count // n_parts
    first_part = me // per_part

    def part_at(index):
        return lax.rem(first_part + index + n_parts // 2, n_parts)

    def term_copy(part):
        return pair_copy(
            term_send.at[part],
            term_recv.at[part],
            term_send_sems.at[part],
            term_recv_sems.at[part],
        )

    def part_term(part, which):
        hidden = hidden_buf[pl.ds(part * per_part, per_part)]
        hidden = hidden.reshape(per_part * cap, gate_ref.shape[1])
        term = jnp.dot(hidden, down_ref[which], preferred_element_type=f32)
        return term.astype(bf16).reshape(per_part, cap, half)

    def back_copy(peer):
        return pltpu.make_async_remote_copy(
            src_ref=result_buf.at[peer],
            dst_ref=back_buf.at[me],
            send_sem=back_send_sems.at[peer],
            recv_sem=back_recv_sems.at[me],
            device_id=(peer, core),
            device_id_type=mesh_ids,
        )

    def back_arrival(peer):
        return pltpu.make_async_remote_copy(
            src_ref=result_buf.at[peer],
            dst_ref=back_buf.at[peer],
            send_sem=back_send_sems.at[peer],
            recv_sem=back_recv_sems.at[peer],
            device_id=(peer, core),
            device_id_type=mesh_ids,
        )

    def send_terms(index, carry):
        part = part_at(index)
        term_send[part] = part_term(part, other)
        term_copy(part).start()
        return carry

    lax.fori_loop(0, n_parts, send_terms, 0)

    def own_terms(index, carry):
        part = part_at(index)
        term_own[part] = part_term(part, core)
        return carry

    lax.fori_loop(0, n_parts, own_terms, 0)

    def finish_part(index, carry):
        part = part_at(index)
        term_copy(part).wait_recv()
        total = term_own[part].astype(f32) + term_recv[part].astype(f32)
        result_buf[pl.ds(part * per_part, per_part)] = total.astype(bf16)

        def start_back(inner, carry_inner):
            peer = part * per_part + inner

            @pl.when(peer != me)
            def _():
                back_copy(peer).start()

            return carry_inner

        lax.fori_loop(0, per_part, start_back, 0)
        return carry

    lax.fori_loop(0, n_parts, finish_part, 0)
    back_buf[me] = result_buf[me]

    def finish_sends(step, carry):
        out_copy(step).wait_send()
        back_arrival(peer_at(step)).wait_recv()
        back_copy(peer_at(step)).wait_send()
        return carry

    lax.fori_loop(1, ep_count, finish_sends, 0)

    def finish_pair(step, carry):
        rows_copy(step).wait_send()
        return carry

    lax.fori_loop(0, ep_count, finish_pair, 0)

    def finish_terms(part, carry):
        term_copy(part).wait_send()
        return carry

    lax.fori_loop(0, n_parts, finish_terms, 0)

    back = back_buf[...].reshape(total_rows, half)
    moe_out = jnp.dot(combine_high, back, preferred_element_type=f32)
    moe_out += jnp.dot(combine_low, back, preferred_element_type=f32)
    moe_ref[...] = moe_out


def shards(
    tokens_in,
    state_in,
    norm_mix,
    w_recept,
    w_key,
    w_value,
    decay_down,
    decay_up,
    decay_base,
    iclr_down,
    iclr_up,
    iclr_base,
    key_scale,
    key_mix,
    w_out,
    norm_moe,
    router_group,
    router_expert,
    routes,
    expert_gate,
    expert_up,
    expert_down,
):
    f32 = jnp.float32
    bf16 = jnp.bfloat16
    seq_count, width_model = tokens_in.shape
    heads_here, head_size = state_in.shape[1], state_in.shape[3]
    channels = heads_here * head_size
    tp_count = lax.axis_size("tp")
    ep_count = lax.axis_size("ep")
    dma = pltpu.SemaphoreType.DMA
    vmem = pl.BlockSpec(memory_space=pltpu.VMEM)
    anywhere = pl.BlockSpec(memory_space=pl.ANY)
    n_chunks = 2 if seq_count % 2 == 0 else 1
    mixed, state_out = pl.pallas_call(
        mixer_kernel,
        out_shape=(
            jax.ShapeDtypeStruct((seq_count, channels), bf16),
            jax.ShapeDtypeStruct(state_in.shape, f32),
        ),
        in_specs=[vmem] * 2 + [anywhere] * 3 + [vmem] * 8 + [anywhere],
        out_specs=(vmem, anywhere),
        scratch_shapes=[
            pltpu.VMEM((3, width_model, channels), bf16),
            pltpu.VMEM(state_in.shape, f32),
            pltpu.VMEM(state_in.shape, f32),
            dma((3,)),
            dma((n_chunks,)),
            dma((n_chunks,)),
        ],
        compiler_params=pltpu.CompilerParams(vmem_limit_bytes=60 * 1024 * 1024),
    )(
        tokens_in,
        norm_mix,
        w_recept,
        w_key,
        w_value,
        decay_down.T,
        decay_up,
        decay_base,
        iclr_down.T,
        iclr_up,
        iclr_base,
        key_scale,
        key_mix,
        state_in,
    )
    top_count = routes.shape[1]
    half_width = width_model // tp_count
    limit = max(2, 2 * seq_count * top_count // ep_count)
    cap = -(-limit // 16) * 16
    block_rows = min(ep_count * cap, 256)
    n_parts = min(4, ep_count)
    per_part = ep_count // n_parts
    hidden_width = expert_gate.shape[2]
    moe_out, mid_half = pl.pallas_call(
        functools.partial(moe_kernel, ep_count, block_rows),
        out_shape=(
            jax.ShapeDtypeStruct((seq_count, half_width), f32),
            jax.ShapeDtypeStruct((seq_count, half_width), bf16),
        ),
        in_specs=[vmem, anywhere] + [vmem] * 5 + [anywhere] * 3,
        out_specs=(vmem, vmem),
        scratch_shapes=[
            pltpu.VMEM((width_model, hidden_width), bf16),
            pltpu.VMEM((width_model, hidden_width), bf16),
            pltpu.VMEM((tp_count, hidden_width, half_width), bf16),
            pltpu.VMEM(w_out.shape, bf16),
            pltpu.VMEM((tp_count, seq_count, half_width), f32),
            pltpu.VMEM((tp_count, seq_count, half_width), f32),
            pltpu.VMEM((tp_count, seq_count, half_width), bf16),
            pltpu.VMEM((tp_count, seq_count, half_width), bf16),
            pltpu.VMEM((ep_count, cap, half_width), bf16),
            pltpu.VMEM((tp_count, ep_count, cap, half_width), bf16),
            pltpu.VMEM((ep_count, cap, hidden_width), bf16),
            pltpu.VMEM((n_parts, per_part, cap, half_width), bf16),
            pltpu.VMEM((n_parts, per_part, cap, half_width), bf16),
            pltpu.VMEM((n_parts, per_part, cap, half_width), bf16),
            pltpu.VMEM((ep_count, cap, half_width), bf16),
            pltpu.VMEM((ep_count, cap, half_width), bf16),
            dma((2,)),
            dma((ep_count,)),
            dma((ep_count,)),
            dma((ep_count,)),
            dma((ep_count,)),
            dma((n_parts,)),
            dma((n_parts,)),
            dma((ep_count,)),
            dma((ep_count,)),
            dma((5,)),
        ],
        compiler_params=pltpu.CompilerParams(
            collective_id=0, has_side_effects=True, vmem_limit_bytes=60 * 1024 * 1024
        ),
    )(
        mixed,
        w_out,
        tokens_in,
        norm_moe,
        router_group.T,
        router_expert.T,
        routes.T,
        expert_gate,
        expert_up,
        expert_down,
    )
    layer_out = (mid_half.astype(f32) + moe_out).astype(bf16)
    return (layer_out, state_out)


def solution(mesh):
    in_specs = (
        P("ep", None),
        P("ep", "tp", None, None),
        P(),
        P(None, "tp"),
        P(None, "tp"),
        P(None, "tp"),
        P(),
        P(None, "tp"),
        P("tp"),
        P(),
        P(None, "tp"),
        P("tp"),
        P("tp"),
        P("tp"),
        P("tp", None),
        P(),
        P(),
        P(),
        P("ep", None),
        P("ep", None, "tp"),
        P("ep", None, "tp"),
        P("ep", "tp", None),
    )
    out_specs = (P("ep", "tp"), P("ep", "tp", None, None))
    return jax.shard_map(shards, mesh=mesh, in_specs=in_specs, out_specs=out_specs, check_vma=False)
```

```python
import functools

import jax
import jax.numpy as jnp
from jax import lax
from jax.experimental import pallas as pl
from jax.experimental.pallas import tpu as pltpu
from jax.sharding import PartitionSpec as P


def mixer_kernel(
    tokens_ref, norm_ref, w_recept_hbm, w_key_hbm, w_value_hbm, decay_down_ref, decay_up_ref, decay_base_ref,
    iclr_down_ref, iclr_up_ref, iclr_base_ref, key_scale_ref, key_mix_ref, state_hbm,
    mixed_ref, state_out_hbm,
    weights, state_buf, out_buf, weight_sems, in_sems, out_sems,
):
    f32 = jnp.float32
    bf16 = jnp.bfloat16
    seq_count, width = tokens_ref.shape
    heads, head_size = state_hbm.shape[1], state_hbm.shape[3]
    channels = heads * head_size
    n_chunks = in_sems.shape[0]
    per_chunk = seq_count // n_chunks
    rows_dims = (((1,), (1,)), ((), ()))
    weight_loads = [
        pltpu.make_async_copy(source, weights.at[index], weight_sems.at[index])
        for index, source in enumerate((w_key_hbm, w_recept_hbm, w_value_hbm))
    ]
    for load in weight_loads:
        load.start()
    state_loads = []
    state_stores = []
    for index in range(n_chunks):
        span = pl.ds(index * per_chunk, per_chunk)
        state_loads.append(
            pltpu.make_async_copy(state_hbm.at[span], state_buf.at[span], in_sems.at[index])
        )
        state_stores.append(
            pltpu.make_async_copy(out_buf.at[span], state_out_hbm.at[span], out_sems.at[index])
        )
        state_loads[index].start()

    tokens = tokens_ref[...].astype(f32)
    factor = lax.rsqrt(jnp.mean(tokens * tokens, axis=1, keepdims=True) + 1e-06)
    normed = (tokens * factor * norm_ref[...].reshape(1, width).astype(f32)).astype(bf16)
    decay_low = jnp.tanh(
        lax.dot_general(normed, decay_down_ref[...], rows_dims, preferred_element_type=f32)
    ).astype(bf16)
    iclr_low = lax.dot_general(
        normed, iclr_down_ref[...], rows_dims, preferred_element_type=f32
    ).astype(bf16)
    decay_in = decay_base_ref[...].reshape(1, channels) + jnp.dot(
        decay_low, decay_up_ref[...], preferred_element_type=f32
    )
    decays = jnp.exp(-jnp.exp(jnp.float32(-0.5)) * jax.nn.sigmoid(decay_in))
    rate = jax.nn.sigmoid(
        iclr_base_ref[...].reshape(1, channels)
        + jnp.dot(iclr_low, iclr_up_ref[...], preferred_element_type=f32)
    )

    def project(index):
        weight_loads[index].wait()
        rows = jnp.dot(normed, weights[index], preferred_element_type=f32)
        return rows.astype(bf16).astype(f32)

    key = project(0)
    scaled = key * key_scale_ref[...].reshape(1, channels).astype(f32)
    key_mod = key * (1.0 + (rate - 1.0) * key_mix_ref[...].reshape(1, channels).astype(f32))
    spans = [slice(head * head_size, (head + 1) * head_size) for head in range(heads)]
    units = []
    for span in spans:
        part = scaled[:, span]
        units.append(part * lax.rsqrt(jnp.sum(part * part, axis=1, keepdims=True) + 1e-06))
    recept = project(1)
    readers, writers, gains = [], [], []
    for head, span in enumerate(spans):
        unit, query = units[head], recept[:, span]
        drop = unit * rate[:, span]
        shift = jnp.sum(drop * query, axis=1, keepdims=True)
        gains.append(jnp.sum(key_mod[:, span] * query, axis=1, keepdims=True))
        reader = decays[:, span] * query - unit * shift
        readers.append(jnp.concatenate([unit, reader], axis=0).astype(bf16))
        writers.append(jnp.concatenate([-drop, key_mod[:, span]], axis=0).astype(bf16))
    value = project(2)
    value_t = jnp.concatenate([value, value], axis=0).T

    lanes = lax.broadcasted_iota(jnp.int32, (per_chunk, head_size, 2 * seq_count), 2)
    seqs = lax.broadcasted_iota(jnp.int32, (per_chunk, head_size, 2 * seq_count), 0)
    first = lanes < seq_count
    owner = jnp.where(first, lanes, lanes - seq_count)
    totals = [jnp.zeros((head_size, 2 * seq_count), f32) for _ in range(heads)]
    for index in range(n_chunks):
        rows = slice(index * per_chunk, (index + 1) * per_chunk)
        here = owner == seqs + index * per_chunk
        state_loads[index].wait()
        for head, span in enumerate(spans):
            state = state_buf[rows, head]
            flat = state.reshape(per_chunk * head_size, head_size).astype(bf16)
            read = lax.dot_general(flat, readers[head], rows_dims, preferred_element_type=f32)
            read = read.reshape(per_chunk, head_size, 2 * seq_count)
            totals[head] += jnp.sum(jnp.where(here, read, 0.0), axis=0)
            terms = jnp.where(here, jnp.where(first, read, value_t[span, :][None]), 0.0)
            terms = terms.reshape(per_chunk * head_size, 2 * seq_count).astype(bf16)
            change = jnp.dot(terms, writers[head], preferred_element_type=f32)
            out_buf[rows, head] = state * decays[rows, span][:, None, :] + change.reshape(
                per_chunk, head_size, head_size
            )
        state_stores[index].start()
    total = jnp.concatenate(totals, axis=0).T[seq_count:]
    for head, span in enumerate(spans):
        mixed_ref[:, span] = (total[:, span] + value[:, span] * gains[head]).astype(bf16)
    for store in state_stores:
        store.wait()


def moe_kernel(
    ep_count,
    mixed_ref,
    w_out_hbm,
    tokens_ref,
    norm_ref,
    router_group_ref,
    router_expert_ref,
    routes_ref,
    gate_hbm,
    up_hbm,
    down_hbm,
    out_ref,
    gate_ref,
    up_ref,
    down_ref,
    w_out_ref,
    part_buf,
    part_recv,
    mid_buf,
    norm_buf,
    place_own,
    place_all,
    comb_own,
    comb_all,
    rows_own,
    rows_all,
    send_buf,
    rows_buf,
    term_send,
    term_recv,
    result_buf,
    back_buf,
    sum_send,
    sum_recv,
    part_sems,
    place_send_sems,
    place_recv_sems,
    comb_send_sems,
    comb_recv_sems,
    cross_send_sems,
    cross_recv_sems,
    fan_send_sems,
    fan_recv_sems,
    pair_send_sems,
    pair_recv_sems,
    term_send_sems,
    term_recv_sems,
    back_send_sems,
    back_recv_sems,
    sum_send_sems,
    sum_recv_sems,
    load_sems,
):
    f32 = jnp.float32
    bf16 = jnp.bfloat16
    me = lax.axis_index("ep")
    core = lax.axis_index("tp")
    other = 1 - core
    seq_count, width = tokens_ref.shape
    half = width // 2
    cap = send_buf.shape[2]
    total_rows = ep_count * cap
    mesh_ids = pl.DeviceIdType.MESH
    n_groups = router_group_ref.shape[0]
    size = ep_count // n_groups
    group = me // size
    rank = me % size
    block_rows = size * cap
    hidden_width = gate_ref.shape[1]
    power = size & (size - 1) == 0
    steps = sorted(range(1, size), key=lambda step: -bin(step).count("1"))

    def flip(step):
        moved = rank * 0
        bit = 1
        while bit < size:
            value = rank // bit % 2
            moved = moved + bit * ((1 - value) if step & bit else value)
            bit *= 2
        return moved

    to_rank = {s: flip(s) if power else (rank + s) % size for s in steps}
    from_rank = {s: flip(s) if power else (rank + size - s) % size for s in steps}
    base = group * size

    def each(low, high, visit):
        if high - low <= 2:
            for index in range(low, high):
                visit(index)
        else:
            lax.fori_loop(low, high, lambda index, carry: (visit(index), carry)[1], 0)

    def source_group(block):
        return (group + n_groups - block) % n_groups

    def target_group(block):
        return (group + block) % n_groups

    def remote(source, target, send_sem, recv_sem, device):
        return pltpu.make_async_remote_copy(
            src_ref=source,
            dst_ref=target,
            send_sem=send_sem,
            recv_sem=recv_sem,
            device_id=device,
            device_id_type=mesh_ids,
        )

    barrier = pltpu.get_barrier_semaphore()

    def greet(device):
        pl.semaphore_signal(barrier, inc=1, device_id=device, device_id_type=mesh_ids)

    each(1, n_groups, lambda block: greet((target_group(block) * size + rank, core)))
    for step in steps:
        greet((base + to_rank[step], core))
    greet((me, other))

    loads = [
        pltpu.make_async_copy(w_out_hbm, w_out_ref, load_sems.at[0]),
        pltpu.make_async_copy(gate_hbm.at[0], gate_ref, load_sems.at[1]),
        pltpu.make_async_copy(up_hbm.at[0], up_ref, load_sems.at[2]),
        pltpu.make_async_copy(down_hbm.at[0, :, pl.ds(0, half)], down_ref.at[0], load_sems.at[3]),
        pltpu.make_async_copy(down_hbm.at[0, :, pl.ds(half, half)], down_ref.at[1], load_sems.at[4]),
    ]
    for load in loads:
        load.start()

    expert_ids = lax.broadcasted_iota(jnp.int32, (ep_count, seq_count), 0)
    uses = jnp.zeros((ep_count, seq_count), f32)
    for index in range(routes_ref.shape[0]):
        uses += jnp.where(routes_ref[index : index + 1, :] == expert_ids, 1.0, 0.0)
    group_ids = lax.broadcasted_iota(jnp.int32, (n_groups, seq_count), 0)
    group_hit = jnp.where(routes_ref[0:1, :] // size == group_ids, 1.0, 0.0)
    row_ids = lax.broadcasted_iota(jnp.int32, (seq_count, seq_count), 0)
    column_ids = lax.broadcasted_iota(jnp.int32, (seq_count, seq_count), 1)
    earlier = jnp.where(row_ids < column_ids, 1.0, 0.0).astype(bf16)
    position = jnp.dot(uses.astype(bf16), earlier, preferred_element_type=f32)
    slots = jnp.where(uses > 0.5, position, -1.0).astype(bf16)
    slot_rows = lax.broadcasted_iota(jnp.int32, (total_rows, ep_count), 0)
    slot_experts = lax.broadcasted_iota(jnp.int32, (total_rows, ep_count), 1)
    spread = jnp.where(slot_rows // cap == slot_experts, 1.0, 0.0).astype(bf16)
    slot_of_row = lax.broadcasted_iota(jnp.int32, (total_rows, seq_count), 0) % cap
    hits = jnp.dot(spread, slots, preferred_element_type=f32) == slot_of_row.astype(f32)
    chooser = jnp.where(hits, 1.0, 0.0)
    place_own[...] = chooser.astype(bf16).reshape(n_groups, block_rows, seq_count)
    place_all[group] = place_own[group]

    loads[0].wait()
    for index in range(2):
        columns = slice(index * half, (index + 1) * half)
        part_buf[index] = jnp.dot(
            mixed_ref[...], w_out_ref[:, columns], preferred_element_type=f32
        )
    pl.semaphore_wait(barrier, (n_groups - 1) + (size - 1) + 1)

    part_copy = remote(part_buf, part_recv, part_sems.at[0], part_sems.at[1], (me, other))
    part_copy.start()

    def across(block, buffer, target, send_sems, recv_sems):
        goal = target_group(block)
        return remote(
            buffer.at[goal] if buffer is not rows_own else buffer,
            target.at[group],
            send_sems.at[block],
            recv_sems.at[group],
            (goal * size + rank, core),
        )

    def across_arrival(block, buffer, target, send_sems, recv_sems):
        origin = source_group(block)
        return remote(
            buffer.at[origin] if buffer is not rows_own else buffer,
            target.at[origin],
            send_sems.at[block],
            recv_sems.at[origin],
            (origin * size + rank, core),
        )

    place_args = (place_own, place_all, place_send_sems, place_recv_sems)
    comb_args = (comb_own, comb_all, comb_send_sems, comb_recv_sems)
    cross_args = (rows_own, rows_all, cross_send_sems, cross_recv_sems)
    each(1, n_groups, lambda block: across(block, *place_args).start())
    part_copy.wait()

    squares = jnp.zeros((seq_count, 1), f32)
    for index in range(2):
        columns = slice(index * half, (index + 1) * half)
        mixer_out = (part_buf[index] + part_recv[index]).astype(bf16)
        mid = (tokens_ref[:, columns].astype(f32) + mixer_out.astype(f32)).astype(bf16)
        mid_buf[index] = mid
        mid32 = mid.astype(f32)
        squares = squares + jnp.sum(mid32 * mid32, axis=1, keepdims=True)
    factor = lax.rsqrt(squares / width + 1e-06)
    for index in range(2):
        columns = slice(index * half, (index + 1) * half)
        norm_buf[index] = (
            mid_buf[index].astype(f32) * factor * norm_ref[columns].reshape(1, half).astype(f32)
        ).astype(bf16)

    rows_own[...] = norm_buf[core]
    each(1, n_groups, lambda block: across(block, *cross_args).start())
    rows_all[group] = rows_own[...]

    def fan_copy(block, step):
        source = source_group(block) * size + rank
        return remote(
            send_buf.at[block, to_rank[step]],
            rows_buf.at[core, source],
            fan_send_sems.at[block, step],
            fan_recv_sems.at[source],
            (base + to_rank[step], core),
        )

    def fan_arrival(block, step):
        source = source_group(block) * size + from_rank[step]
        return remote(
            send_buf.at[block, to_rank[step]],
            rows_buf.at[core, source],
            fan_send_sems.at[block, step],
            fan_recv_sems.at[source],
            (base + from_rank[step], core),
        )

    def rows_copy(source):
        return remote(
            rows_buf.at[core, source],
            rows_buf.at[core, source],
            pair_send_sems.at[source],
            pair_recv_sems.at[source],
            (me, other),
        )

    def rows_arrival(source):
        return remote(
            rows_buf.at[other, source],
            rows_buf.at[other, source],
            pair_send_sems.at[source],
            pair_recv_sems.at[source],
            (me, other),
        )

    def fan_out(block):
        origin = source_group(block)
        rows = jnp.dot(place_all[origin], rows_all[origin], preferred_element_type=f32)
        send_buf[block] = rows.astype(bf16).reshape(size, cap, half)
        for step in steps:
            fan_copy(block, step).start()
        rows_buf[core, origin * size + rank] = send_buf[block, rank]
        rows_copy(origin * size + rank).start()

    fan_out(0)

    rows_dims = (((1,), (1,)), ((), ()))
    group_logit = jnp.zeros(group_hit.shape, f32)
    expert_logit = jnp.zeros(uses.shape, f32)
    for index in range(2):
        columns = slice(index * half, (index + 1) * half)
        group_logit += lax.dot_general(
            router_group_ref[:, columns], norm_buf[index], rows_dims, preferred_element_type=f32
        )
        expert_logit += lax.dot_general(
            router_expert_ref[:, columns], norm_buf[index], rows_dims, preferred_element_type=f32
        )
    group_prob = jax.nn.sigmoid(jnp.sum(group_logit * group_hit, axis=0, keepdims=True))
    scores = jax.nn.sigmoid(expert_logit) * uses
    weights = group_prob * scores / jnp.sum(scores, axis=0, keepdims=True)
    combine = jnp.dot(spread, weights.astype(bf16), preferred_element_type=f32) * chooser
    combine = combine.T.astype(bf16)
    for index in range(n_groups):
        comb_own[index] = combine[:, index * block_rows : (index + 1) * block_rows]
    comb_all[group] = comb_own[group]
    each(1, n_groups, lambda block: across(block, *comb_args).start())

    def relay_out(block):
        across_arrival(block, *place_args).wait_recv()
        across_arrival(block, *cross_args).wait_recv()
        fan_out(block)

    each(1, n_groups, relay_out)
    for load in loads[1:]:
        load.wait()

    def term_copy(block):
        return remote(
            term_send.at[block],
            term_recv.at[block],
            term_send_sems.at[block],
            term_recv_sems.at[block],
            (me, other),
        )

    def back_copy(block, step):
        return remote(
            result_buf.at[block, to_rank[step]],
            back_buf.at[block, rank],
            back_send_sems.at[block, step],
            back_recv_sems.at[block, rank],
            (base + to_rank[step], core),
        )

    def back_arrival(block, step):
        return remote(
            result_buf.at[block, to_rank[step]],
            back_buf.at[block, from_rank[step]],
            back_send_sems.at[block, step],
            back_recv_sems.at[block, from_rank[step]],
            (base + from_rank[step], core),
        )

    def experts(block):
        first = source_group(block) * size
        for step in reversed(steps):
            fan_arrival(block, step).wait_recv()
            rows_copy(first + from_rank[step]).start()
        for index in range(size):
            rows_arrival(first + index).wait_recv()
        gate_part = jnp.zeros((block_rows, hidden_width), f32)
        up_part = jnp.zeros((block_rows, hidden_width), f32)
        for piece in range(2):
            columns = slice(piece * half, (piece + 1) * half)
            rows = rows_buf[piece, pl.ds(first, size)].reshape(block_rows, half)
            gate_part += jnp.dot(rows, gate_ref[columns, :], preferred_element_type=f32)
            up_part += jnp.dot(rows, up_ref[columns, :], preferred_element_type=f32)
        hidden = (gate_part / (1.0 + jnp.exp(-gate_part)) * up_part).astype(bf16)
        term_send[block] = jnp.dot(
            hidden, down_ref[other], preferred_element_type=f32
        ).astype(bf16)
        term_copy(block).start()
        term = jnp.dot(hidden, down_ref[core], preferred_element_type=f32).astype(bf16)
        term_copy(block).wait_recv()
        total = term.astype(f32) + term_recv[block].astype(f32)
        result_buf[block] = total.astype(bf16).reshape(size, cap, half)
        for step in steps:
            back_copy(block, step).start()
        back_buf[block, rank] = result_buf[block, rank]

    each(0, n_groups, experts)

    def gather(block):
        for step in reversed(steps):
            back_arrival(block, step).wait_recv()
        back = back_buf[block].reshape(block_rows, half)
        return jnp.dot(comb_all[source_group(block)], back, preferred_element_type=f32)

    def sum_copy(block):
        origin = source_group(block)
        return remote(
            sum_send.at[block],
            sum_recv.at[group],
            sum_send_sems.at[block],
            sum_recv_sems.at[group],
            (origin * size + rank, core),
        )

    def sum_arrival(block):
        origin = source_group(block)
        return remote(
            sum_send.at[block],
            sum_recv.at[origin],
            sum_send_sems.at[block],
            sum_recv_sems.at[origin],
            (origin * size + rank, core),
        )

    def return_sum(block):
        across_arrival(block, *comb_args).wait_recv()
        sum_send[block] = gather(block).astype(bf16)
        sum_copy(block).start()

    each(1, n_groups, return_sum)
    part_buf[0] = mid_buf[core].astype(f32) + gather(0)

    def finish_sends(block):
        for step in steps:
            fan_copy(block, step).wait_send()
            back_copy(block, step).wait_send()
        for index in range(size):
            rows_copy(source_group(block) * size + index).wait_send()
        term_copy(block).wait_send()

    each(0, n_groups, finish_sends)

    def finish_cross(block):
        across(block, *place_args).wait_send()
        across(block, *comb_args).wait_send()
        across(block, *cross_args).wait_send()
        sum_copy(block).wait_send()
        sum_arrival(block).wait_recv()
        part_buf[0] += sum_recv[source_group(block)].astype(f32)

    each(1, n_groups, finish_cross)
    out_ref[...] = part_buf[0].astype(bf16)


def shards(
    tokens_in,
    state_in,
    norm_mix,
    w_recept,
    w_key,
    w_value,
    decay_down,
    decay_up,
    decay_base,
    iclr_down,
    iclr_up,
    iclr_base,
    key_scale,
    key_mix,
    w_out,
    norm_moe,
    router_group,
    router_expert,
    routes,
    expert_gate,
    expert_up,
    expert_down,
):
    f32 = jnp.float32
    bf16 = jnp.bfloat16
    seq_count, width_model = tokens_in.shape
    heads_here, head_size = state_in.shape[1], state_in.shape[3]
    channels = heads_here * head_size
    tp_count = lax.axis_size("tp")
    ep_count = lax.axis_size("ep")
    dma = pltpu.SemaphoreType.DMA
    vmem = pl.BlockSpec(memory_space=pltpu.VMEM)
    anywhere = pl.BlockSpec(memory_space=pl.ANY)
    n_chunks = 2 if seq_count % 2 == 0 else 1
    mixed, state_out = pl.pallas_call(
        mixer_kernel,
        out_shape=(
            jax.ShapeDtypeStruct((seq_count, channels), bf16),
            jax.ShapeDtypeStruct(state_in.shape, f32),
        ),
        in_specs=[vmem] * 2 + [anywhere] * 3 + [vmem] * 8 + [anywhere],
        out_specs=(vmem, anywhere),
        scratch_shapes=[
            pltpu.VMEM((3, width_model, channels), bf16),
            pltpu.VMEM(state_in.shape, f32),
            pltpu.VMEM(state_in.shape, f32),
            dma((3,)),
            dma((n_chunks,)),
            dma((n_chunks,)),
        ],
        compiler_params=pltpu.CompilerParams(vmem_limit_bytes=60 * 1024 * 1024),
    )(
        tokens_in,
        norm_mix,
        w_recept,
        w_key,
        w_value,
        decay_down.T,
        decay_up,
        decay_base,
        iclr_down.T,
        iclr_up,
        iclr_base,
        key_scale,
        key_mix,
        state_in,
    )
    top_count = routes.shape[1]
    half_width = width_model // tp_count
    limit = max(2, 2 * seq_count * top_count // ep_count)
    cap = -(-limit // 16) * 16
    n_groups = router_group.shape[1]
    size = ep_count // n_groups
    block_rows = size * cap
    hidden_width = expert_gate.shape[2]
    layer_out = pl.pallas_call(
        functools.partial(moe_kernel, ep_count),
        out_shape=jax.ShapeDtypeStruct((seq_count, half_width), bf16),
        in_specs=[vmem, anywhere] + [vmem] * 5 + [anywhere] * 3,
        out_specs=vmem,
        scratch_shapes=[
            pltpu.VMEM((width_model, hidden_width), bf16),
            pltpu.VMEM((width_model, hidden_width), bf16),
            pltpu.VMEM((tp_count, hidden_width, half_width), bf16),
            pltpu.VMEM(w_out.shape, bf16),
            pltpu.VMEM((tp_count, seq_count, half_width), f32),
            pltpu.VMEM((tp_count, seq_count, half_width), f32),
            pltpu.VMEM((tp_count, seq_count, half_width), bf16),
            pltpu.VMEM((tp_count, seq_count, half_width), bf16),
            pltpu.VMEM((n_groups, block_rows, seq_count), bf16),
            pltpu.VMEM((n_groups, block_rows, seq_count), bf16),
            pltpu.VMEM((n_groups, seq_count, block_rows), bf16),
            pltpu.VMEM((n_groups, seq_count, block_rows), bf16),
            pltpu.VMEM((seq_count, half_width), bf16),
            pltpu.VMEM((n_groups, seq_count, half_width), bf16),
            pltpu.VMEM((n_groups, size, cap, half_width), bf16),
            pltpu.VMEM((tp_count, ep_count, cap, half_width), bf16),
            pltpu.VMEM((n_groups, block_rows, half_width), bf16),
            pltpu.VMEM((n_groups, block_rows, half_width), bf16),
            pltpu.VMEM((n_groups, size, cap, half_width), bf16),
            pltpu.VMEM((n_groups, size, cap, half_width), bf16),
            pltpu.VMEM((n_groups, seq_count, half_width), bf16),
            pltpu.VMEM((n_groups, seq_count, half_width), bf16),
            dma((2,)),
            dma((n_groups,)),
            dma((n_groups,)),
            dma((n_groups,)),
            dma((n_groups,)),
            dma((n_groups,)),
            dma((n_groups,)),
            dma((n_groups, size)),
            dma((ep_count,)),
            dma((ep_count,)),
            dma((ep_count,)),
            dma((n_groups,)),
            dma((n_groups,)),
            dma((n_groups, size)),
            dma((n_groups, size)),
            dma((n_groups,)),
            dma((n_groups,)),
            dma((5,)),
        ],
        compiler_params=pltpu.CompilerParams(
            collective_id=0, has_side_effects=True, vmem_limit_bytes=60 * 1024 * 1024
        ),
    )(
        mixed,
        w_out,
        tokens_in,
        norm_moe,
        router_group.T,
        router_expert.T,
        routes.T,
        expert_gate,
        expert_up,
        expert_down,
    )
    return (layer_out, state_out)


def solution(mesh):
    in_specs = (
        P("ep", None),
        P("ep", "tp", None, None),
        P(),
        P(None, "tp"),
        P(None, "tp"),
        P(None, "tp"),
        P(),
        P(None, "tp"),
        P("tp"),
        P(),
        P(None, "tp"),
        P("tp"),
        P("tp"),
        P("tp"),
        P("tp", None),
        P(),
        P(),
        P(),
        P("ep", None),
        P("ep", None, "tp"),
        P("ep", None, "tp"),
        P("ep", "tp", None),
    )
    out_specs = (P("ep", "tp"), P("ep", "tp", None, None))
    return jax.shard_map(shards, mesh=mesh, in_specs=in_specs, out_specs=out_specs, check_vma=False)
```

```python
import functools

import jax
import jax.numpy as jnp
from jax import lax
from jax.experimental import pallas as pl
from jax.experimental.pallas import tpu as pltpu
from jax.sharding import PartitionSpec as P


def layer_kernel(
    ep_count,
    tokens_ref,
    norm_mix_ref,
    w_recept_hbm,
    w_key_hbm,
    w_value_hbm,
    decay_down_ref,
    decay_up_ref,
    decay_base_ref,
    iclr_down_ref,
    iclr_up_ref,
    iclr_base_ref,
    key_scale_ref,
    key_mix_ref,
    state_hbm,
    w_out_hbm,
    norm_ref,
    router_group_ref,
    router_expert_ref,
    routes_ref,
    gate_hbm,
    up_hbm,
    down_hbm,
    out_ref,
    state_out_ref,
    weights,
    state_buf,
    terms_buf,
    decay_buf,
    writer_buf,
    gate_ref,
    up_ref,
    down_ref,
    w_out_ref,
    part_buf,
    part_recv,
    mid_buf,
    norm_buf,
    place_own,
    place_all,
    comb_own,
    comb_all,
    rows_own,
    rows_all,
    send_buf,
    rows_buf,
    term_send,
    term_recv,
    result_buf,
    back_buf,
    sum_send,
    sum_recv,
    part_sems,
    place_send_sems,
    place_recv_sems,
    comb_send_sems,
    comb_recv_sems,
    cross_send_sems,
    cross_recv_sems,
    fan_send_sems,
    fan_recv_sems,
    pair_send_sems,
    pair_recv_sems,
    term_send_sems,
    term_recv_sems,
    back_send_sems,
    back_recv_sems,
    sum_send_sems,
    sum_recv_sems,
    load_sems,
    weight_sems,
    in_sems,
):
    f32 = jnp.float32
    bf16 = jnp.bfloat16
    me = lax.axis_index("ep")
    core = lax.axis_index("tp")
    other = 1 - core
    seq_count, width = tokens_ref.shape
    half = width // 2
    heads, head_size = state_hbm.shape[1], state_hbm.shape[3]
    channels = heads * head_size
    rows_dims = (((1,), (1,)), ((), ()))
    cap = send_buf.shape[2]
    total_rows = ep_count * cap
    mesh_ids = pl.DeviceIdType.MESH
    n_groups = router_group_ref.shape[0]
    size = ep_count // n_groups
    group = me // size
    rank = me % size
    block_rows = size * cap
    hidden_width = gate_ref.shape[1]
    power = size & (size - 1) == 0
    steps = sorted(range(1, size), key=lambda step: -bin(step).count("1"))

    def flip(step):
        moved = rank * 0
        bit = 1
        while bit < size:
            value = rank // bit % 2
            moved = moved + bit * ((1 - value) if step & bit else value)
            bit *= 2
        return moved

    to_rank = {s: flip(s) if power else (rank + s) % size for s in steps}
    from_rank = {s: flip(s) if power else (rank + size - s) % size for s in steps}
    base = group * size

    def each(low, high, visit):
        if high - low <= 2:
            for index in range(low, high):
                visit(index)
        else:
            lax.fori_loop(low, high, lambda index, carry: (visit(index), carry)[1], 0)

    def source_group(block):
        return (group + n_groups - block) % n_groups

    def target_group(block):
        return (group + block) % n_groups

    def remote(source, target, send_sem, recv_sem, device):
        return pltpu.make_async_remote_copy(
            src_ref=source,
            dst_ref=target,
            send_sem=send_sem,
            recv_sem=recv_sem,
            device_id=device,
            device_id_type=mesh_ids,
        )

    barrier = pltpu.get_barrier_semaphore()

    def greet(device):
        pl.semaphore_signal(barrier, inc=1, device_id=device, device_id_type=mesh_ids)

    each(1, n_groups, lambda block: greet((target_group(block) * size + rank, core)))
    for step in steps:
        greet((base + to_rank[step], core))
    greet((me, other))

    loads = [
        pltpu.make_async_copy(w_out_hbm, w_out_ref, load_sems.at[0]),
        pltpu.make_async_copy(gate_hbm.at[0], gate_ref, load_sems.at[1]),
        pltpu.make_async_copy(up_hbm.at[0], up_ref, load_sems.at[2]),
        pltpu.make_async_copy(down_hbm.at[0, :, pl.ds(0, half)], down_ref.at[0], load_sems.at[3]),
        pltpu.make_async_copy(down_hbm.at[0, :, pl.ds(half, half)], down_ref.at[1], load_sems.at[4]),
    ]
    weight_loads = [
        pltpu.make_async_copy(source, weights.at[index], weight_sems.at[index])
        for index, source in enumerate((w_key_hbm, w_recept_hbm, w_value_hbm))
    ]
    for load in weight_loads:
        load.start()
    n_chunks = in_sems.shape[0]
    per_chunk = seq_count // n_chunks
    state_loads = []
    for index in range(n_chunks):
        span = pl.ds(index * per_chunk, per_chunk)
        state_loads.append(
            pltpu.make_async_copy(state_hbm.at[span], state_buf.at[span], in_sems.at[index])
        )
        state_loads[index].start()
    for load in loads:
        load.start()

    tokens = tokens_ref[...].astype(f32)
    factor = lax.rsqrt(jnp.mean(tokens * tokens, axis=1, keepdims=True) + 1e-06)
    normed = (tokens * factor * norm_mix_ref[...].reshape(1, width).astype(f32)).astype(bf16)
    decay_low = jnp.tanh(
        lax.dot_general(normed, decay_down_ref[...], rows_dims, preferred_element_type=f32)
    ).astype(bf16)
    iclr_low = lax.dot_general(
        normed, iclr_down_ref[...], rows_dims, preferred_element_type=f32
    ).astype(bf16)
    decay_in = decay_base_ref[...].reshape(1, channels) + jnp.dot(
        decay_low, decay_up_ref[...], preferred_element_type=f32
    )
    decays = jnp.exp(-jnp.exp(jnp.float32(-0.5)) * jax.nn.sigmoid(decay_in))
    rate = jax.nn.sigmoid(
        iclr_base_ref[...].reshape(1, channels)
        + jnp.dot(iclr_low, iclr_up_ref[...], preferred_element_type=f32)
    )

    def project(index):
        weight_loads[index].wait()
        rows = jnp.dot(normed, weights[index], preferred_element_type=f32)
        return rows.astype(bf16).astype(f32)

    key = project(0)
    scaled = key * key_scale_ref[...].reshape(1, channels).astype(f32)
    key_mod = key * (1.0 + (rate - 1.0) * key_mix_ref[...].reshape(1, channels).astype(f32))
    spans = [slice(head * head_size, (head + 1) * head_size) for head in range(heads)]
    units = []
    for span in spans:
        part = scaled[:, span]
        units.append(part * lax.rsqrt(jnp.sum(part * part, axis=1, keepdims=True) + 1e-06))
    recept = project(1)
    readers, writers, gains = [], [], []
    for head, span in enumerate(spans):
        unit, query = units[head], recept[:, span]
        drop = unit * rate[:, span]
        shift = jnp.sum(drop * query, axis=1, keepdims=True)
        gains.append(jnp.sum(key_mod[:, span] * query, axis=1, keepdims=True))
        reader = decays[:, span] * query - unit * shift
        readers.append(jnp.concatenate([unit, reader], axis=0).astype(bf16))
        writers.append(jnp.concatenate([-drop, key_mod[:, span]], axis=0).astype(bf16))
    value = project(2)
    value_t = jnp.concatenate([value, value], axis=0).T

    lanes = lax.broadcasted_iota(jnp.int32, (per_chunk, head_size, 2 * seq_count), 2)
    seqs = lax.broadcasted_iota(jnp.int32, (per_chunk, head_size, 2 * seq_count), 0)
    first = lanes < seq_count
    owner = jnp.where(first, lanes, lanes - seq_count)
    totals = [jnp.zeros((head_size, 2 * seq_count), f32) for _ in range(heads)]
    for index in range(n_chunks):
        rows = slice(index * per_chunk, (index + 1) * per_chunk)
        here = owner == seqs + index * per_chunk
        state_loads[index].wait()
        for head, span in enumerate(spans):
            flat = state_buf[rows, head].reshape(per_chunk * head_size, head_size).astype(bf16)
            read = lax.dot_general(flat, readers[head], rows_dims, preferred_element_type=f32)
            read = read.reshape(per_chunk, head_size, 2 * seq_count)
            totals[head] += jnp.sum(jnp.where(here, read, 0.0), axis=0)
            terms = jnp.where(here, jnp.where(first, read, value_t[span, :][None]), 0.0)
            terms_buf[head, rows] = terms.astype(bf16)
    total = jnp.concatenate(totals, axis=0).T[seq_count:]
    mixed = [total[:, span] + value[:, span] * gains[head] for head, span in enumerate(spans)]
    mixed = jnp.concatenate(mixed, axis=1).astype(bf16)
    for head, span in enumerate(spans):
        decay_buf[head] = decays[:, span]
        writer_buf[head] = writers[head]

    expert_ids = lax.broadcasted_iota(jnp.int32, (ep_count, seq_count), 0)
    uses = jnp.zeros((ep_count, seq_count), f32)
    for index in range(routes_ref.shape[0]):
        uses += jnp.where(routes_ref[index : index + 1, :] == expert_ids, 1.0, 0.0)
    group_ids = lax.broadcasted_iota(jnp.int32, (n_groups, seq_count), 0)
    group_hit = jnp.where(routes_ref[0:1, :] // size == group_ids, 1.0, 0.0)
    row_ids = lax.broadcasted_iota(jnp.int32, (seq_count, seq_count), 0)
    column_ids = lax.broadcasted_iota(jnp.int32, (seq_count, seq_count), 1)
    earlier = jnp.where(row_ids < column_ids, 1.0, 0.0).astype(bf16)
    position = jnp.dot(uses.astype(bf16), earlier, preferred_element_type=f32)
    slots = jnp.where(uses > 0.5, position, -1.0).astype(bf16)
    slot_rows = lax.broadcasted_iota(jnp.int32, (total_rows, ep_count), 0)
    slot_experts = lax.broadcasted_iota(jnp.int32, (total_rows, ep_count), 1)
    spread = jnp.where(slot_rows // cap == slot_experts, 1.0, 0.0).astype(bf16)
    slot_of_row = lax.broadcasted_iota(jnp.int32, (total_rows, seq_count), 0) % cap
    hits = jnp.dot(spread, slots, preferred_element_type=f32) == slot_of_row.astype(f32)
    chooser = jnp.where(hits, 1.0, 0.0)
    place_own[...] = chooser.astype(bf16).reshape(n_groups, block_rows, seq_count)
    place_all[group] = place_own[group]

    loads[0].wait()
    for index in range(2):
        columns = slice(index * half, (index + 1) * half)
        part_buf[index] = jnp.dot(
            mixed, w_out_ref[:, columns], preferred_element_type=f32
        )
    pl.semaphore_wait(barrier, (n_groups - 1) + (size - 1) + 1)

    part_copy = remote(part_buf, part_recv, part_sems.at[0], part_sems.at[1], (me, other))
    part_copy.start()

    def across(block, buffer, target, send_sems, recv_sems):
        goal = target_group(block)
        return remote(
            buffer.at[goal] if buffer is not rows_own else buffer,
            target.at[group],
            send_sems.at[block],
            recv_sems.at[group],
            (goal * size + rank, core),
        )

    def across_arrival(block, buffer, target, send_sems, recv_sems):
        origin = source_group(block)
        return remote(
            buffer.at[origin] if buffer is not rows_own else buffer,
            target.at[origin],
            send_sems.at[block],
            recv_sems.at[origin],
            (origin * size + rank, core),
        )

    place_args = (place_own, place_all, place_send_sems, place_recv_sems)
    comb_args = (comb_own, comb_all, comb_send_sems, comb_recv_sems)
    cross_args = (rows_own, rows_all, cross_send_sems, cross_recv_sems)
    each(1, n_groups, lambda block: across(block, *place_args).start())
    part_copy.wait()

    squares = jnp.zeros((seq_count, 1), f32)
    for index in range(2):
        columns = slice(index * half, (index + 1) * half)
        mixer_out = (part_buf[index] + part_recv[index]).astype(bf16)
        mid = (tokens_ref[:, columns].astype(f32) + mixer_out.astype(f32)).astype(bf16)
        mid_buf[index] = mid
        mid32 = mid.astype(f32)
        squares = squares + jnp.sum(mid32 * mid32, axis=1, keepdims=True)
    factor = lax.rsqrt(squares / width + 1e-06)
    for index in range(2):
        columns = slice(index * half, (index + 1) * half)
        norm_buf[index] = (
            mid_buf[index].astype(f32) * factor * norm_ref[columns].reshape(1, half).astype(f32)
        ).astype(bf16)

    rows_own[...] = norm_buf[core]
    each(1, n_groups, lambda block: across(block, *cross_args).start())
    rows_all[group] = rows_own[...]

    def fan_copy(block, step):
        source = source_group(block) * size + rank
        return remote(
            send_buf.at[block, to_rank[step]],
            rows_buf.at[core, source],
            fan_send_sems.at[block, step],
            fan_recv_sems.at[source],
            (base + to_rank[step], core),
        )

    def fan_arrival(block, step):
        source = source_group(block) * size + from_rank[step]
        return remote(
            send_buf.at[block, to_rank[step]],
            rows_buf.at[core, source],
            fan_send_sems.at[block, step],
            fan_recv_sems.at[source],
            (base + from_rank[step], core),
        )

    def rows_copy(source):
        return remote(
            rows_buf.at[core, source],
            rows_buf.at[core, source],
            pair_send_sems.at[source],
            pair_recv_sems.at[source],
            (me, other),
        )

    def rows_arrival(source):
        return remote(
            rows_buf.at[other, source],
            rows_buf.at[other, source],
            pair_send_sems.at[source],
            pair_recv_sems.at[source],
            (me, other),
        )

    def fan_out(block):
        origin = source_group(block)
        rows = jnp.dot(place_all[origin], rows_all[origin], preferred_element_type=f32)
        send_buf[block] = rows.astype(bf16).reshape(size, cap, half)
        for step in steps:
            fan_copy(block, step).start()
        rows_buf[core, origin * size + rank] = send_buf[block, rank]
        rows_copy(origin * size + rank).start()

    fan_out(0)

    group_logit = jnp.zeros(group_hit.shape, f32)
    expert_logit = jnp.zeros(uses.shape, f32)
    for index in range(2):
        columns = slice(index * half, (index + 1) * half)
        group_logit += lax.dot_general(
            router_group_ref[:, columns], norm_buf[index], rows_dims, preferred_element_type=f32
        )
        expert_logit += lax.dot_general(
            router_expert_ref[:, columns], norm_buf[index], rows_dims, preferred_element_type=f32
        )
    group_prob = jax.nn.sigmoid(jnp.sum(group_logit * group_hit, axis=0, keepdims=True))
    scores = jax.nn.sigmoid(expert_logit) * uses
    route_weights = group_prob * scores / jnp.sum(scores, axis=0, keepdims=True)
    combine = jnp.dot(spread, route_weights.astype(bf16), preferred_element_type=f32) * chooser
    combine = combine.T.astype(bf16)
    for index in range(n_groups):
        comb_own[index] = combine[:, index * block_rows : (index + 1) * block_rows]
    comb_all[group] = comb_own[group]
    each(1, n_groups, lambda block: across(block, *comb_args).start())

    def update_state():
        for index in range(n_chunks):
            rows = slice(index * per_chunk, (index + 1) * per_chunk)
            for head in range(heads):
                terms = terms_buf[head, rows].reshape(per_chunk * head_size, 2 * seq_count)
                change = jnp.dot(terms, writer_buf[head], preferred_element_type=f32)
                state_out_ref[rows, head] = state_buf[rows, head] * decay_buf[head, rows][
                    :, None, :
                ] + change.reshape(per_chunk, head_size, head_size)

    update_state()

    def relay_out(block):
        across_arrival(block, *place_args).wait_recv()
        across_arrival(block, *cross_args).wait_recv()
        fan_out(block)

    each(1, n_groups, relay_out)
    for load in loads[1:]:
        load.wait()

    def term_copy(block):
        return remote(
            term_send.at[block],
            term_recv.at[block],
            term_send_sems.at[block],
            term_recv_sems.at[block],
            (me, other),
        )

    def back_copy(block, step):
        return remote(
            result_buf.at[block, to_rank[step]],
            back_buf.at[block, rank],
            back_send_sems.at[block, step],
            back_recv_sems.at[block, rank],
            (base + to_rank[step], core),
        )

    def back_arrival(block, step):
        return remote(
            result_buf.at[block, to_rank[step]],
            back_buf.at[block, from_rank[step]],
            back_send_sems.at[block, step],
            back_recv_sems.at[block, from_rank[step]],
            (base + from_rank[step], core),
        )

    def experts(block):
        first = source_group(block) * size
        for step in reversed(steps):
            fan_arrival(block, step).wait_recv()
            rows_copy(first + from_rank[step]).start()
        for index in range(size):
            rows_arrival(first + index).wait_recv()
        gate_part = jnp.zeros((block_rows, hidden_width), f32)
        up_part = jnp.zeros((block_rows, hidden_width), f32)
        for piece in range(2):
            columns = slice(piece * half, (piece + 1) * half)
            rows = rows_buf[piece, pl.ds(first, size)].reshape(block_rows, half)
            gate_part += jnp.dot(rows, gate_ref[columns, :], preferred_element_type=f32)
            up_part += jnp.dot(rows, up_ref[columns, :], preferred_element_type=f32)
        hidden = (gate_part / (1.0 + jnp.exp(-gate_part)) * up_part).astype(bf16)
        term_send[block] = jnp.dot(
            hidden, down_ref[other], preferred_element_type=f32
        ).astype(bf16)
        term_copy(block).start()
        term = jnp.dot(hidden, down_ref[core], preferred_element_type=f32).astype(bf16)
        term_copy(block).wait_recv()
        total = term.astype(f32) + term_recv[block].astype(f32)
        result_buf[block] = total.astype(bf16).reshape(size, cap, half)
        for step in steps:
            back_copy(block, step).start()
        back_buf[block, rank] = result_buf[block, rank]

    each(0, n_groups, experts)

    def gather(block):
        for step in reversed(steps):
            back_arrival(block, step).wait_recv()
        back = back_buf[block].reshape(block_rows, half)
        return jnp.dot(comb_all[source_group(block)], back, preferred_element_type=f32)

    def sum_copy(block):
        origin = source_group(block)
        return remote(
            sum_send.at[block],
            sum_recv.at[group],
            sum_send_sems.at[block],
            sum_recv_sems.at[group],
            (origin * size + rank, core),
        )

    def sum_arrival(block):
        origin = source_group(block)
        return remote(
            sum_send.at[block],
            sum_recv.at[origin],
            sum_send_sems.at[block],
            sum_recv_sems.at[origin],
            (origin * size + rank, core),
        )

    def return_sum(block):
        across_arrival(block, *comb_args).wait_recv()
        sum_send[block] = gather(block).astype(bf16)
        sum_copy(block).start()

    each(1, n_groups, return_sum)
    part_buf[0] = mid_buf[core].astype(f32) + gather(0)

    def finish_sends(block):
        for step in steps:
            fan_copy(block, step).wait_send()
            back_copy(block, step).wait_send()
        for index in range(size):
            rows_copy(source_group(block) * size + index).wait_send()
        term_copy(block).wait_send()

    each(0, n_groups, finish_sends)

    def finish_cross(block):
        across(block, *place_args).wait_send()
        across(block, *comb_args).wait_send()
        across(block, *cross_args).wait_send()
        sum_copy(block).wait_send()
        sum_arrival(block).wait_recv()
        part_buf[0] += sum_recv[source_group(block)].astype(f32)

    each(1, n_groups, finish_cross)
    out_ref[...] = part_buf[0].astype(bf16)


def shards(
    tokens_in,
    state_in,
    norm_mix,
    w_recept,
    w_key,
    w_value,
    decay_down,
    decay_up,
    decay_base,
    iclr_down,
    iclr_up,
    iclr_base,
    key_scale,
    key_mix,
    w_out,
    norm_moe,
    router_group,
    router_expert,
    routes,
    expert_gate,
    expert_up,
    expert_down,
):
    f32 = jnp.float32
    bf16 = jnp.bfloat16
    seq_count, width_model = tokens_in.shape
    heads_here, head_size = state_in.shape[1], state_in.shape[3]
    channels = heads_here * head_size
    tp_count = lax.axis_size("tp")
    ep_count = lax.axis_size("ep")
    dma = pltpu.SemaphoreType.DMA
    vmem = pl.BlockSpec(memory_space=pltpu.VMEM)
    anywhere = pl.BlockSpec(memory_space=pl.ANY)
    n_chunks = 2 if seq_count % 2 == 0 else 1
    top_count = routes.shape[1]
    half_width = width_model // tp_count
    limit = max(2, 2 * seq_count * top_count // ep_count)
    cap = -(-limit // 16) * 16
    n_groups = router_group.shape[1]
    size = ep_count // n_groups
    block_rows = size * cap
    hidden_width = expert_gate.shape[2]
    block_bytes = ep_count * cap * width_model
    vmem_limit = min(58 * 1024 * 1024, 24 * 1024 * 1024 + 10 * block_bytes)
    layer = pl.pallas_call(
        functools.partial(layer_kernel, ep_count),
        out_shape=(
            jax.ShapeDtypeStruct((seq_count, half_width), bf16),
            jax.ShapeDtypeStruct(state_in.shape, f32),
        ),
        in_specs=[vmem] * 2
        + [anywhere] * 3
        + [vmem] * 8
        + [anywhere] * 2
        + [vmem] * 4
        + [anywhere] * 3,
        out_specs=(vmem, vmem),
        scratch_shapes=[
            pltpu.VMEM((3, width_model, channels), bf16),
            pltpu.VMEM(state_in.shape, f32),
            pltpu.VMEM((heads_here, seq_count, head_size, 2 * seq_count), bf16),
            pltpu.VMEM((heads_here, seq_count, head_size), f32),
            pltpu.VMEM((heads_here, 2 * seq_count, head_size), bf16),
            pltpu.VMEM((width_model, hidden_width), bf16),
            pltpu.VMEM((width_model, hidden_width), bf16),
            pltpu.VMEM((tp_count, hidden_width, half_width), bf16),
            pltpu.VMEM(w_out.shape, bf16),
            pltpu.VMEM((tp_count, seq_count, half_width), f32),
            pltpu.VMEM((tp_count, seq_count, half_width), f32),
            pltpu.VMEM((tp_count, seq_count, half_width), bf16),
            pltpu.VMEM((tp_count, seq_count, half_width), bf16),
            pltpu.VMEM((n_groups, block_rows, seq_count), bf16),
            pltpu.VMEM((n_groups, block_rows, seq_count), bf16),
            pltpu.VMEM((n_groups, seq_count, block_rows), bf16),
            pltpu.VMEM((n_groups, seq_count, block_rows), bf16),
            pltpu.VMEM((seq_count, half_width), bf16),
            pltpu.VMEM((n_groups, seq_count, half_width), bf16),
            pltpu.VMEM((n_groups, size, cap, half_width), bf16),
            pltpu.VMEM((tp_count, ep_count, cap, half_width), bf16),
            pltpu.VMEM((n_groups, block_rows, half_width), bf16),
            pltpu.VMEM((n_groups, block_rows, half_width), bf16),
            pltpu.VMEM((n_groups, size, cap, half_width), bf16),
            pltpu.VMEM((n_groups, size, cap, half_width), bf16),
            pltpu.VMEM((n_groups, seq_count, half_width), bf16),
            pltpu.VMEM((n_groups, seq_count, half_width), bf16),
            dma((2,)),
            dma((n_groups,)),
            dma((n_groups,)),
            dma((n_groups,)),
            dma((n_groups,)),
            dma((n_groups,)),
            dma((n_groups,)),
            dma((n_groups, size)),
            dma((ep_count,)),
            dma((ep_count,)),
            dma((ep_count,)),
            dma((n_groups,)),
            dma((n_groups,)),
            dma((n_groups, size)),
            dma((n_groups, size)),
            dma((n_groups,)),
            dma((n_groups,)),
            dma((5,)),
            dma((3,)),
            dma((n_chunks,)),
        ],
        compiler_params=pltpu.CompilerParams(
            collective_id=0, has_side_effects=True, vmem_limit_bytes=vmem_limit
        ),
    )
    operands = (
        tokens_in, norm_mix, w_recept, w_key, w_value, decay_down.T, decay_up, decay_base,
        iclr_down.T, iclr_up, iclr_base, key_scale, key_mix, state_in, w_out, norm_moe,
        router_group.T, router_expert.T, routes.T, expert_gate, expert_up, expert_down,
    )
    layer_out, state_out = layer(
        *(pltpu.with_memory_space_constraint(operand, pltpu.HBM) for operand in operands)
    )
    return (layer_out, state_out)


def solution(mesh):
    in_specs = (
        P("ep", None),
        P("ep", "tp", None, None),
        P(),
        P(None, "tp"),
        P(None, "tp"),
        P(None, "tp"),
        P(),
        P(None, "tp"),
        P("tp"),
        P(),
        P(None, "tp"),
        P("tp"),
        P("tp"),
        P("tp"),
        P("tp", None),
        P(),
        P(),
        P(),
        P("ep", None),
        P("ep", None, "tp"),
        P("ep", None, "tp"),
        P("ep", "tp", None),
    )
    out_specs = (P("ep", "tp"), P("ep", "tp", None, None))
    return jax.shard_map(shards, mesh=mesh, in_specs=in_specs, out_specs=out_specs, check_vma=False)
```

```python
import functools

import jax
import jax.numpy as jnp
from jax import lax
from jax.experimental import pallas as pl
from jax.experimental.pallas import tpu as pltpu
from jax.sharding import PartitionSpec as P


def layer_kernel(
    ep_count,
    tokens_hbm,
    routes_hbm,
    norm_mix_hbm,
    decay_down_hbm,
    iclr_down_hbm,
    decay_up_hbm,
    decay_base_hbm,
    iclr_up_hbm,
    iclr_base_hbm,
    key_scale_hbm,
    key_mix_hbm,
    norm_moe_hbm,
    router_group_hbm,
    router_expert_hbm,
    w_recept_hbm,
    w_key_hbm,
    w_value_hbm,
    state_hbm,
    w_out_hbm,
    gate_hbm,
    up_hbm,
    down_hbm,
    out_ref,
    state_out_ref,
    tokens_ref,
    routes_ref,
    norm_mix_ref,
    decay_down_ref,
    iclr_down_ref,
    decay_up_ref,
    decay_base_ref,
    iclr_up_ref,
    iclr_base_ref,
    key_scale_ref,
    key_mix_ref,
    norm_ref,
    router_group_ref,
    router_expert_ref,
    weights,
    state_buf,
    terms_buf,
    decay_buf,
    writer_buf,
    w_out_ref,
    first_ref,
    down_ref,
    part_buf,
    part_recv,
    mid_buf,
    norm_buf,
    place_own,
    place_all,
    comb_own,
    comb_all,
    rows_own,
    rows_all,
    send_buf,
    rows_buf,
    sums_own,
    sums_recv,
    result_buf,
    back_buf,
    total_send,
    total_recv,
    small_sems,
    weight_sems,
    in_sems,
    load_sems,
    share_send_sems,
    share_recv_sems,
    part_sems,
    place_send_sems,
    place_recv_sems,
    comb_send_sems,
    comb_recv_sems,
    cross_send_sems,
    cross_recv_sems,
    fan_send_sems,
    fan_recv_sems,
    sums_send_sems,
    sums_recv_sems,
    back_send_sems,
    back_recv_sems,
    total_send_sems,
    total_recv_sems,
):
    f32 = jnp.float32
    bf16 = jnp.bfloat16
    me = lax.axis_index("ep")
    core = lax.axis_index("tp")
    other = 1 - core
    seq_count, width = tokens_ref.shape
    half = width // 2
    heads, head_size = state_hbm.shape[1], state_hbm.shape[3]
    channels = heads * head_size
    rows_dims = (((1,), (1,)), ((), ()))
    cap = send_buf.shape[2]
    total_rows = ep_count * cap
    mesh_ids = pl.DeviceIdType.MESH
    n_groups = router_group_ref.shape[0]
    size = ep_count // n_groups
    group = me // size
    rank = me % size
    base = group * size
    block_rows = size * cap
    hidden_part = gate_hbm.shape[2]
    hidden_width = 2 * hidden_part
    power = size & (size - 1) == 0
    steps = sorted(range(1, size), key=lambda step: -bin(step).count("1"))
    near = [step for step in steps if 2 * step < size]
    far = [step for step in steps if 2 * step >= size]

    def flip(step):
        moved = rank * 0
        bit = 1
        while bit < size:
            value = rank // bit % 2
            moved = moved + bit * ((1 - value) if step & bit else value)
            bit *= 2
        return moved

    to_rank = {s: flip(s) if power else (rank + s) % size for s in steps}
    from_rank = {s: flip(s) if power else (rank + size - s) % size for s in steps}

    def each(low, high, visit):
        if high - low <= 2:
            for index in range(low, high):
                visit(index)
        else:
            lax.fori_loop(low, high, lambda index, carry: (visit(index), carry)[1], 0)

    def source_group(block):
        return (group + n_groups - block) % n_groups

    def target_group(block):
        return (group + block) % n_groups

    def remote(source, target, send_sem, recv_sem, device):
        return pltpu.make_async_remote_copy(
            src_ref=source,
            dst_ref=target,
            send_sem=send_sem,
            recv_sem=recv_sem,
            device_id=device,
            device_id_type=mesh_ids,
        )

    partner = (me, other)
    barrier = pltpu.get_barrier_semaphore()

    def greet(device):
        pl.semaphore_signal(barrier, inc=1, device_id=device, device_id_type=mesh_ids)

    each(1, n_groups, lambda block: greet((target_group(block) * size + rank, core)))
    for step in steps:
        greet((base + to_rank[step], core))
    greet(partner)

    small = [
        pltpu.make_async_copy(source, target, small_sems.at[index])
        for index, (source, target) in enumerate(
            (
                (tokens_hbm, tokens_ref),
                (routes_hbm, routes_ref),
                (norm_mix_hbm, norm_mix_ref),
                (decay_down_hbm, decay_down_ref),
                (iclr_down_hbm, iclr_down_ref),
                (decay_up_hbm, decay_up_ref),
                (decay_base_hbm, decay_base_ref),
                (iclr_up_hbm, iclr_up_ref),
                (iclr_base_hbm, iclr_base_ref),
                (key_scale_hbm, key_scale_ref),
                (key_mix_hbm, key_mix_ref),
                (norm_moe_hbm, norm_ref),
                (router_group_hbm, router_group_ref),
                (router_expert_hbm, router_expert_ref),
            )
        )
    ]
    for load in small:
        load.start()
    weight_loads = [
        pltpu.make_async_copy(source, weights.at[index], weight_sems.at[index])
        for index, source in enumerate((w_key_hbm, w_recept_hbm, w_value_hbm))
    ]
    for load in weight_loads:
        load.start()
    n_chunks = in_sems.shape[0]
    per_chunk = seq_count // n_chunks
    state_loads = []
    for index in range(n_chunks):
        span = pl.ds(index * per_chunk, per_chunk)
        state_loads.append(
            pltpu.make_async_copy(state_hbm.at[span], state_buf.at[span], in_sems.at[index])
        )

    def columns_of(which):
        return pl.ds(pl.multiple_of(which * half, half), half)

    hidden_here = pl.ds(pl.multiple_of(core * hidden_part, hidden_part), hidden_part)
    shared = (
        (lambda which: gate_hbm.at[0, columns_of(which)], first_ref.at[0, :, hidden_here]),
        (lambda which: up_hbm.at[0, columns_of(which)], first_ref.at[1, :, hidden_here]),
        (lambda which: down_hbm.at[0, :, columns_of(which)], down_ref.at[hidden_here]),
    )
    loads = [pltpu.make_async_copy(w_out_hbm, w_out_ref, load_sems.at[0])]
    shares = []
    for index, (source, target) in enumerate(shared):
        loads.append(pltpu.make_async_copy(source(core), target, load_sems.at[1 + index]))
        shares.append(
            remote(
                source(other), target, share_send_sems.at[index], share_recv_sems.at[index], partner
            )
        )
    for load in small[:2]:
        load.wait()

    expert_ids = lax.broadcasted_iota(jnp.int32, (ep_count, seq_count), 0)
    uses = jnp.zeros((ep_count, seq_count), f32)
    for index in range(routes_ref.shape[0]):
        uses += jnp.where(routes_ref[index : index + 1, :] == expert_ids, 1.0, 0.0)
    group_ids = lax.broadcasted_iota(jnp.int32, (n_groups, seq_count), 0)
    group_hit = jnp.where(routes_ref[0:1, :] // size == group_ids, 1.0, 0.0)
    row_ids = lax.broadcasted_iota(jnp.int32, (seq_count, seq_count), 0)
    column_ids = lax.broadcasted_iota(jnp.int32, (seq_count, seq_count), 1)
    earlier = jnp.where(row_ids < column_ids, 1.0, 0.0).astype(bf16)
    position = jnp.dot(uses.astype(bf16), earlier, preferred_element_type=f32)
    slots = jnp.where(uses > 0.5, position, -1.0).astype(bf16)
    slot_rows = lax.broadcasted_iota(jnp.int32, (total_rows, ep_count), 0)
    slot_experts = lax.broadcasted_iota(jnp.int32, (total_rows, ep_count), 1)
    spread = jnp.where(slot_rows // cap == slot_experts, 1.0, 0.0).astype(bf16)
    slot_of_row = lax.broadcasted_iota(jnp.int32, (total_rows, seq_count), 0) % cap
    hits = jnp.dot(spread, slots, preferred_element_type=f32) == slot_of_row.astype(f32)
    chooser = jnp.where(hits, 1.0, 0.0)
    place_own[...] = chooser.astype(bf16).reshape(n_groups, block_rows, seq_count)
    place_all[group] = place_own[group]

    def across(block, source, target, send_sems, recv_sems):
        return remote(
            source,
            target.at[group],
            send_sems.at[block],
            recv_sems.at[group],
            (target_group(block) * size + rank, core),
        )

    def across_arrival(block, source, target, send_sems, recv_sems):
        origin = source_group(block)
        return remote(
            source,
            target.at[origin],
            send_sems.at[block],
            recv_sems.at[origin],
            (origin * size + rank, core),
        )

    def place_args(block):
        return (block, place_own.at[target_group(block)], place_all, place_send_sems, place_recv_sems)

    def comb_args(block):
        return (block, comb_own.at[target_group(block)], comb_all, comb_send_sems, comb_recv_sems)

    def cross_args(block):
        return (block, rows_own, rows_all, cross_send_sems, cross_recv_sems)

    def sum_args(block):
        return (block, total_send.at[block], total_recv, total_send_sems, total_recv_sems)

    def fan_copy(block, step):
        return remote(
            send_buf.at[block, to_rank[step]],
            rows_buf.at[block, rank],
            fan_send_sems.at[block, step],
            fan_recv_sems.at[block, rank],
            (base + to_rank[step], core),
        )

    def fan_arrival(block, step):
        return remote(
            send_buf.at[block, to_rank[step]],
            rows_buf.at[block, from_rank[step]],
            fan_send_sems.at[block, step],
            fan_recv_sems.at[block, from_rank[step]],
            (base + from_rank[step], core),
        )

    def fan_out(block):
        origin = source_group(block)
        rows = jnp.dot(place_all[origin], rows_all[origin], preferred_element_type=f32)
        send_buf[block] = rows.astype(bf16).reshape(size, cap, half)
        rows_buf[block, rank] = send_buf[block, rank]

    def fan_start(block, chosen):
        for step in chosen:
            fan_copy(block, step).start()

    for load in state_loads:
        load.start()

    for load in small[2:5]:
        load.wait()
    tokens = tokens_ref[...].astype(f32)
    factor = lax.rsqrt(jnp.mean(tokens * tokens, axis=1, keepdims=True) + 1e-06)
    normed = (tokens * factor * norm_mix_ref[...].reshape(1, width).astype(f32)).astype(bf16)
    decay_low = jnp.tanh(
        lax.dot_general(normed, decay_down_ref[...], rows_dims, preferred_element_type=f32)
    ).astype(bf16)
    iclr_low = lax.dot_general(
        normed, iclr_down_ref[...], rows_dims, preferred_element_type=f32
    ).astype(bf16)
    for load in small[5:]:
        load.wait()
    decay_in = decay_base_ref[...].reshape(1, channels) + jnp.dot(
        decay_low, decay_up_ref[...], preferred_element_type=f32
    )
    decays = jnp.exp(-jnp.exp(jnp.float32(-0.5)) * jax.nn.sigmoid(decay_in))
    rate = jax.nn.sigmoid(
        iclr_base_ref[...].reshape(1, channels)
        + jnp.dot(iclr_low, iclr_up_ref[...], preferred_element_type=f32)
    )

    def project(index):
        weight_loads[index].wait()
        rows = jnp.dot(normed, weights[index], preferred_element_type=f32)
        return rows.astype(bf16).astype(f32)

    key = project(0)
    scaled = key * key_scale_ref[...].reshape(1, channels).astype(f32)
    key_mod = key * (1.0 + (rate - 1.0) * key_mix_ref[...].reshape(1, channels).astype(f32))
    spans = [slice(head * head_size, (head + 1) * head_size) for head in range(heads)]
    units = []
    for span in spans:
        part = scaled[:, span]
        units.append(part * lax.rsqrt(jnp.sum(part * part, axis=1, keepdims=True) + 1e-06))
    recept = project(1)
    readers, writers, gains = [], [], []
    for head, span in enumerate(spans):
        unit, query = units[head], recept[:, span]
        drop = unit * rate[:, span]
        shift = jnp.sum(drop * query, axis=1, keepdims=True)
        gains.append(jnp.sum(key_mod[:, span] * query, axis=1, keepdims=True))
        reader = decays[:, span] * query - unit * shift
        readers.append(jnp.concatenate([unit, reader], axis=0).astype(bf16))
        writers.append(jnp.concatenate([-drop, key_mod[:, span]], axis=0).astype(bf16))
    value = project(2)
    value_t = jnp.concatenate([value, value], axis=0).T
    for load in loads:
        load.start()
    pl.semaphore_wait(barrier, (n_groups - 1) + (size - 1) + 1)
    for share in shares:
        share.start()
    each(1, n_groups, lambda block: across(*place_args(block)).start())

    def relay_rows(block):
        across_arrival(*cross_args(block)).wait_recv()
        across_arrival(*place_args(block)).wait_recv()
        fan_out(block)
        fan_start(block, steps)

    lanes = lax.broadcasted_iota(jnp.int32, (per_chunk, head_size, 2 * seq_count), 2)
    seqs = lax.broadcasted_iota(jnp.int32, (per_chunk, head_size, 2 * seq_count), 0)
    first = lanes < seq_count
    owner = jnp.where(first, lanes, lanes - seq_count)
    totals = [jnp.zeros((head_size, 2 * seq_count), f32) for _ in range(heads)]
    for index in range(n_chunks):
        rows = slice(index * per_chunk, (index + 1) * per_chunk)
        here = owner == seqs + index * per_chunk
        state_loads[index].wait()
        for head, span in enumerate(spans):
            flat = state_buf[rows, head].reshape(per_chunk * head_size, head_size).astype(bf16)
            read = lax.dot_general(flat, readers[head], rows_dims, preferred_element_type=f32)
            read = read.reshape(per_chunk, head_size, 2 * seq_count)
            totals[head] += jnp.sum(jnp.where(here, read, 0.0), axis=0)
            terms = jnp.where(here, jnp.where(first, read, value_t[span, :][None]), 0.0)
            terms_buf[head, rows] = terms.astype(bf16)
    total = jnp.concatenate(totals, axis=0).T[seq_count:]
    mixed = [total[:, span] + value[:, span] * gains[head] for head, span in enumerate(spans)]
    mixed = jnp.concatenate(mixed, axis=1).astype(bf16)
    for head, span in enumerate(spans):
        decay_buf[head] = decays[:, span]
        writer_buf[head] = writers[head]

    loads[0].wait()
    for index in range(2):
        columns = slice(index * half, (index + 1) * half)
        part_buf[index] = jnp.dot(mixed, w_out_ref[:, columns], preferred_element_type=f32)
    part_copy = remote(part_buf, part_recv, part_sems.at[0], part_sems.at[1], partner)
    part_copy.start()

    def update_state():
        for index in range(n_chunks):
            rows = slice(index * per_chunk, (index + 1) * per_chunk)
            for head in range(heads):
                terms = terms_buf[head, rows].reshape(per_chunk * head_size, 2 * seq_count)
                change = jnp.dot(terms, writer_buf[head], preferred_element_type=f32)
                state_out_ref[rows, head] = state_buf[rows, head] * decay_buf[head, rows][
                    :, None, :
                ] + change.reshape(per_chunk, head_size, head_size)

    part_copy.wait()

    squares = jnp.zeros((seq_count, 1), f32)
    for index in range(2):
        columns = slice(index * half, (index + 1) * half)
        mixer_out = (part_buf[index] + part_recv[index]).astype(bf16)
        mid = (tokens_ref[:, columns].astype(f32) + mixer_out.astype(f32)).astype(bf16)
        mid_buf[index] = mid
        mid32 = mid.astype(f32)
        squares = squares + jnp.sum(mid32 * mid32, axis=1, keepdims=True)
    factor = lax.rsqrt(squares / width + 1e-06)
    for index in range(2):
        columns = slice(index * half, (index + 1) * half)
        norm_buf[index] = (
            mid_buf[index].astype(f32) * factor * norm_ref[columns].reshape(1, half).astype(f32)
        ).astype(bf16)
    rows_own[...] = norm_buf[core]
    each(1, n_groups, lambda block: across(*cross_args(block)).start())
    rows_all[group] = rows_own[...]
    fan_out(0)
    fan_start(0, steps)
    group_logit = jnp.zeros(group_hit.shape, f32)
    expert_logit = jnp.zeros(uses.shape, f32)
    for index in range(2):
        columns = slice(index * half, (index + 1) * half)
        group_logit += lax.dot_general(
            router_group_ref[:, columns], norm_buf[index], rows_dims, preferred_element_type=f32
        )
        expert_logit += lax.dot_general(
            router_expert_ref[:, columns], norm_buf[index], rows_dims, preferred_element_type=f32
        )
    group_prob = jax.nn.sigmoid(jnp.sum(group_logit * group_hit, axis=0, keepdims=True))
    scores = jax.nn.sigmoid(expert_logit) * uses
    route_weights = group_prob * scores / jnp.sum(scores, axis=0, keepdims=True)
    combine = jnp.dot(spread, route_weights.astype(bf16), preferred_element_type=f32) * chooser
    combine = combine.T.astype(bf16)
    for index in range(n_groups):
        comb_own[index] = combine[:, index * block_rows : (index + 1) * block_rows]
    comb_all[group] = comb_own[group]
    each(1, n_groups, lambda block: across(*comb_args(block)).start())

    update_state()
    each(1, n_groups, relay_rows)
    for load in loads[1:]:
        load.wait()
    for share in shares:
        share.wait_recv()
    def sums_copy(block):
        return remote(
            sums_own.at[block],
            sums_recv.at[block],
            sums_send_sems.at[block],
            sums_recv_sems.at[block],
            partner,
        )

    def first_products(block):
        for step in reversed(steps):
            fan_arrival(block, step).wait_recv()
        rows = rows_buf[block].reshape(block_rows, half)
        for index in range(2):
            sums_own[block, :, index * hidden_width : (index + 1) * hidden_width] = jnp.dot(
                rows, first_ref[index], preferred_element_type=f32
            )
        sums_copy(block).start()

    def back_copy(block, step):
        return remote(
            result_buf.at[block, to_rank[step]],
            back_buf.at[block, rank],
            back_send_sems.at[block, step],
            back_recv_sems.at[block, rank],
            (base + to_rank[step], core),
        )

    def back_arrival(block, step):
        return remote(
            result_buf.at[block, to_rank[step]],
            back_buf.at[block, from_rank[step]],
            back_send_sems.at[block, step],
            back_recv_sems.at[block, from_rank[step]],
            (base + from_rank[step], core),
        )

    def second_product(block):
        sums_copy(block).wait_recv()
        sums = sums_own[block] + sums_recv[block]
        gate_part = sums[:, :hidden_width]
        up_part = sums[:, hidden_width:]
        hidden = (gate_part / (1.0 + jnp.exp(-gate_part)) * up_part).astype(bf16)
        result = jnp.dot(hidden, down_ref[...], preferred_element_type=f32)
        result_buf[block] = result.astype(bf16).reshape(size, cap, half)
        for step in steps:
            back_copy(block, step).start()
        back_buf[block, rank] = result_buf[block, rank]

    first_products(0)
    second_product(0)
    each(1, n_groups, first_products)
    each(1, n_groups, second_product)

    def gather(block):
        for step in reversed(steps):
            back_arrival(block, step).wait_recv()
        back = back_buf[block].reshape(block_rows, half)
        return jnp.dot(comb_all[source_group(block)], back, preferred_element_type=f32)

    def sum_copy(block):
        origin = source_group(block)
        return remote(
            total_send.at[block],
            total_recv.at[group],
            total_send_sems.at[block],
            total_recv_sems.at[group],
            (origin * size + rank, core),
        )

    def return_sum(block):
        across_arrival(*comb_args(block)).wait_recv()
        total_send[block] = gather(block).astype(bf16)
        sum_copy(block).start()

    each(1, n_groups, return_sum)
    part_buf[0] = mid_buf[core].astype(f32) + gather(0)

    def add_sum(block):
        across_arrival(*sum_args(block)).wait_recv()
        part_buf[0] += total_recv[source_group(block)].astype(f32)

    each(1, n_groups, add_sum)
    out_ref[...] = part_buf[0].astype(bf16)

    def finish_block(block):
        for step in steps:
            fan_copy(block, step).wait_send()
            back_copy(block, step).wait_send()
        sums_copy(block).wait_send()

    each(0, n_groups, finish_block)

    def finish_cross(block):
        across(*place_args(block)).wait_send()
        across(*cross_args(block)).wait_send()
        across(*comb_args(block)).wait_send()
        sum_copy(block).wait_send()

    each(1, n_groups, finish_cross)
    for share in shares:
        share.wait_send()


def shards(
    tokens_in,
    state_in,
    norm_mix,
    w_recept,
    w_key,
    w_value,
    decay_down,
    decay_up,
    decay_base,
    iclr_down,
    iclr_up,
    iclr_base,
    key_scale,
    key_mix,
    w_out,
    norm_moe,
    router_group,
    router_expert,
    routes,
    expert_gate,
    expert_up,
    expert_down,
):
    f32 = jnp.float32
    bf16 = jnp.bfloat16
    seq_count, width_model = tokens_in.shape
    heads_here, head_size = state_in.shape[1], state_in.shape[3]
    channels = heads_here * head_size
    tp_count = lax.axis_size("tp")
    ep_count = lax.axis_size("ep")
    dma = pltpu.SemaphoreType.DMA
    vmem = pl.BlockSpec(memory_space=pltpu.VMEM)
    anywhere = pl.BlockSpec(memory_space=pl.ANY)
    n_chunks = 2 if seq_count % 2 == 0 else 1
    top_count = routes.shape[1]
    half_width = width_model // tp_count
    limit = max(2, 2 * seq_count * top_count // ep_count)
    cap = -(-limit // 16) * 16
    n_groups = router_group.shape[1]
    size = ep_count // n_groups
    block_rows = size * cap
    hidden_width = expert_gate.shape[2]
    block_bytes = ep_count * cap * width_model
    vmem_limit = min(58 * 1024 * 1024, 24 * 1024 * 1024 + 10 * block_bytes)
    vmem_of = pltpu.VMEM
    small = (
        tokens_in, routes.T, norm_mix, decay_down.T, iclr_down.T, decay_up, decay_base,
        iclr_up, iclr_base, key_scale, key_mix, norm_moe, router_group.T, router_expert.T,
    )
    large = (
        w_recept, w_key, w_value, state_in, w_out, expert_gate, expert_up, expert_down,
    )
    operands = small + large
    layer = pl.pallas_call(
        functools.partial(layer_kernel, ep_count),
        out_shape=(
            jax.ShapeDtypeStruct((seq_count, half_width), bf16),
            jax.ShapeDtypeStruct(state_in.shape, f32),
        ),
        in_specs=[anywhere] * len(operands),
        out_specs=(vmem, vmem),
        scratch_shapes=[vmem_of(operand.shape, operand.dtype) for operand in small]
        + [
            vmem_of((3, width_model, channels), bf16),
            vmem_of(state_in.shape, f32),
            vmem_of((heads_here, seq_count, head_size, 2 * seq_count), bf16),
            vmem_of((heads_here, seq_count, head_size), f32),
            vmem_of((heads_here, 2 * seq_count, head_size), bf16),
            vmem_of(w_out.shape, bf16),
            vmem_of((2, half_width, tp_count * hidden_width), bf16),
            vmem_of((tp_count * hidden_width, half_width), bf16),
            vmem_of((tp_count, seq_count, half_width), f32),
            vmem_of((tp_count, seq_count, half_width), f32),
            vmem_of((tp_count, seq_count, half_width), bf16),
            vmem_of((tp_count, seq_count, half_width), bf16),
            vmem_of((n_groups, block_rows, seq_count), bf16),
            vmem_of((n_groups, block_rows, seq_count), bf16),
            vmem_of((n_groups, seq_count, block_rows), bf16),
            vmem_of((n_groups, seq_count, block_rows), bf16),
            vmem_of((seq_count, half_width), bf16),
            vmem_of((n_groups, seq_count, half_width), bf16),
            vmem_of((n_groups, size, cap, half_width), bf16),
            vmem_of((n_groups, size, cap, half_width), bf16),
            vmem_of((n_groups, block_rows, 2 * tp_count * hidden_width), f32),
            vmem_of((n_groups, block_rows, 2 * tp_count * hidden_width), f32),
            vmem_of((n_groups, size, cap, half_width), bf16),
            vmem_of((n_groups, size, cap, half_width), bf16),
            vmem_of((n_groups, seq_count, half_width), bf16),
            vmem_of((n_groups, seq_count, half_width), bf16),
            dma((len(small),)),
            dma((3,)),
            dma((n_chunks,)),
            dma((4,)),
            dma((3,)),
            dma((3,)),
            dma((2,)),
            dma((n_groups,)),
            dma((n_groups,)),
            dma((n_groups,)),
            dma((n_groups,)),
            dma((n_groups,)),
            dma((n_groups,)),
            dma((n_groups, size)),
            dma((n_groups, size)),
            dma((n_groups,)),
            dma((n_groups,)),
            dma((n_groups, size)),
            dma((n_groups, size)),
            dma((n_groups,)),
            dma((n_groups,)),
        ],
        compiler_params=pltpu.CompilerParams(
            collective_id=0, has_side_effects=True, vmem_limit_bytes=vmem_limit
        ),
    )
    layer_out, state_out = layer(
        *(pltpu.with_memory_space_constraint(operand, pltpu.HBM) for operand in operands)
    )
    return (layer_out, state_out)


def solution(mesh):
    in_specs = (
        P("ep", None),
        P("ep", "tp", None, None),
        P(),
        P(None, "tp"),
        P(None, "tp"),
        P(None, "tp"),
        P(),
        P(None, "tp"),
        P("tp"),
        P(),
        P(None, "tp"),
        P("tp"),
        P("tp"),
        P("tp"),
        P("tp", None),
        P(),
        P(),
        P(),
        P("ep", None),
        P("ep", None, "tp"),
        P("ep", None, "tp"),
        P("ep", "tp", None),
    )
    out_specs = (P("ep", "tp"), P("ep", "tp", None, None))
    return jax.shard_map(shards, mesh=mesh, in_specs=in_specs, out_specs=out_specs, check_vma=False)
```

```python
import functools

import jax
import jax.numpy as jnp
from jax import lax
from jax.experimental import pallas as pl
from jax.experimental.pallas import tpu as pltpu
from jax.sharding import PartitionSpec as P


def layer_kernel(
    ep_count,
    tokens_hbm,
    routes_hbm,
    norm_mix_hbm,
    decay_down_hbm,
    iclr_down_hbm,
    decay_up_hbm,
    decay_base_hbm,
    iclr_up_hbm,
    iclr_base_hbm,
    key_scale_hbm,
    key_mix_hbm,
    norm_moe_hbm,
    router_group_hbm,
    router_expert_hbm,
    w_recept_hbm,
    w_key_hbm,
    w_value_hbm,
    state_hbm,
    w_out_hbm,
    gate_hbm,
    up_hbm,
    down_hbm,
    out_ref,
    state_out_ref,
    tokens_ref,
    routes_ref,
    norm_mix_ref,
    decay_down_ref,
    iclr_down_ref,
    decay_up_ref,
    decay_base_ref,
    iclr_up_ref,
    iclr_base_ref,
    key_scale_ref,
    key_mix_ref,
    norm_ref,
    router_group_ref,
    router_expert_ref,
    weights,
    state_buf,
    terms_buf,
    decay_buf,
    writer_buf,
    w_cols,
    first_ref,
    down_ref,
    final_buf,
    logit_own,
    logit_recv,
    place_own,
    place_all,
    comb_own,
    comb_all,
    tokens_own,
    tokens_all,
    mix_own,
    mix_all,
    rows_all,
    send_buf,
    rows_buf,
    sums_own,
    sums_recv,
    result_buf,
    back_buf,
    total_send,
    total_recv,
    small_sems,
    weight_sems,
    in_sems,
    load_sems,
    share_send_sems,
    share_recv_sems,
    logit_sems,
    place_send_sems,
    place_recv_sems,
    comb_send_sems,
    comb_recv_sems,
    cross_send_sems,
    cross_recv_sems,
    mix_send_sems,
    mix_recv_sems,
    fan_send_sems,
    fan_recv_sems,
    sums_send_sems,
    sums_recv_sems,
    back_send_sems,
    back_recv_sems,
    total_send_sems,
    total_recv_sems,
):
    f32 = jnp.float32
    bf16 = jnp.bfloat16
    me = lax.axis_index("ep")
    core = lax.axis_index("tp")
    other = 1 - core
    seq_count, width = tokens_ref.shape
    half = width // 2
    heads, head_size = state_hbm.shape[1], state_hbm.shape[3]
    channels = heads * head_size
    rows_dims = (((1,), (1,)), ((), ()))
    cap = send_buf.shape[2]
    total_rows = ep_count * cap
    mesh_ids = pl.DeviceIdType.MESH
    n_groups = router_group_ref.shape[0]
    size = ep_count // n_groups
    group = me // size
    rank = me % size
    base = group * size
    block_rows = size * cap
    hidden_part = gate_hbm.shape[2]
    hidden_width = 2 * hidden_part
    power = size & (size - 1) == 0
    steps = sorted(range(1, size), key=lambda step: -bin(step).count("1"))
    near = [step for step in steps if 2 * step < size]
    far = [step for step in steps if 2 * step >= size]

    def flip(step):
        moved = rank * 0
        bit = 1
        while bit < size:
            value = rank // bit % 2
            moved = moved + bit * ((1 - value) if step & bit else value)
            bit *= 2
        return moved

    to_rank = {s: flip(s) if power else (rank + s) % size for s in steps}
    from_rank = {s: flip(s) if power else (rank + size - s) % size for s in steps}

    def each(low, high, visit):
        if high - low <= 2:
            for index in range(low, high):
                visit(index)
        else:
            lax.fori_loop(low, high, lambda index, carry: (visit(index), carry)[1], 0)

    def source_group(block):
        return (group + n_groups - block) % n_groups

    def target_group(block):
        return (group + block) % n_groups

    def remote(source, target, send_sem, recv_sem, device):
        return pltpu.make_async_remote_copy(
            src_ref=source,
            dst_ref=target,
            send_sem=send_sem,
            recv_sem=recv_sem,
            device_id=device,
            device_id_type=mesh_ids,
        )

    partner = (me, other)
    pieces = (slice(0, half // 2), slice(half // 2, half))
    barrier = pltpu.get_barrier_semaphore()

    def greet(device):
        pl.semaphore_signal(barrier, inc=1, device_id=device, device_id_type=mesh_ids)

    for which in (core, other):
        each(1, n_groups, lambda block: greet((target_group(block) * size + rank, which)))
    for step in steps:
        greet((base + to_rank[step], core))
    greet(partner)

    small = [
        pltpu.make_async_copy(source, target, small_sems.at[index])
        for index, (source, target) in enumerate(
            (
                (tokens_hbm, tokens_ref),
                (routes_hbm, routes_ref),
                (norm_mix_hbm, norm_mix_ref),
                (decay_down_hbm, decay_down_ref),
                (iclr_down_hbm, iclr_down_ref),
                (decay_up_hbm, decay_up_ref),
                (decay_base_hbm, decay_base_ref),
                (iclr_up_hbm, iclr_up_ref),
                (iclr_base_hbm, iclr_base_ref),
                (key_scale_hbm, key_scale_ref),
                (key_mix_hbm, key_mix_ref),
                (norm_moe_hbm, norm_ref),
                (router_group_hbm, router_group_ref),
                (router_expert_hbm, router_expert_ref),
            )
        )
    ]
    for load in small:
        load.start()
    weight_loads = [
        pltpu.make_async_copy(source, weights.at[index], weight_sems.at[index])
        for index, source in enumerate((w_key_hbm, w_recept_hbm, w_value_hbm))
    ]
    for load in weight_loads:
        load.start()
    n_chunks = in_sems.shape[0]
    per_chunk = seq_count // n_chunks
    state_loads = []
    for index in range(n_chunks):
        span = pl.ds(index * per_chunk, per_chunk)
        state_loads.append(
            pltpu.make_async_copy(state_hbm.at[span], state_buf.at[span], in_sems.at[index])
        )

    def columns_of(which):
        return pl.ds(pl.multiple_of(which * half, half), half)

    hidden_here = pl.ds(pl.multiple_of(core * hidden_part, hidden_part), hidden_part)
    shared = (
        (lambda which: w_out_hbm.at[:, columns_of(which)], w_cols.at[core]),
        (lambda which: gate_hbm.at[0, columns_of(which)], first_ref.at[0, :, hidden_here]),
        (lambda which: up_hbm.at[0, columns_of(which)], first_ref.at[1, :, hidden_here]),
        (lambda which: down_hbm.at[0, :, columns_of(which)], down_ref.at[hidden_here]),
    )
    loads = []
    shares = []
    for index, (source, target) in enumerate(shared):
        loads.append(pltpu.make_async_copy(source(core), target, load_sems.at[index]))
        shares.append(
            remote(
                source(other), target, share_send_sems.at[index], share_recv_sems.at[index], partner
            )
        )
    for load in small[:2]:
        load.wait()

    expert_ids = lax.broadcasted_iota(jnp.int32, (ep_count, seq_count), 0)
    uses = jnp.zeros((ep_count, seq_count), f32)
    for index in range(routes_ref.shape[0]):
        uses += jnp.where(routes_ref[index : index + 1, :] == expert_ids, 1.0, 0.0)
    group_ids = lax.broadcasted_iota(jnp.int32, (n_groups, seq_count), 0)
    group_hit = jnp.where(routes_ref[0:1, :] // size == group_ids, 1.0, 0.0)
    row_ids = lax.broadcasted_iota(jnp.int32, (seq_count, seq_count), 0)
    column_ids = lax.broadcasted_iota(jnp.int32, (seq_count, seq_count), 1)
    earlier = jnp.where(row_ids < column_ids, 1.0, 0.0).astype(bf16)
    position = jnp.dot(uses.astype(bf16), earlier, preferred_element_type=f32)
    slots = jnp.where(uses > 0.5, position, -1.0).astype(bf16)
    slot_rows = lax.broadcasted_iota(jnp.int32, (total_rows, ep_count), 0)
    slot_experts = lax.broadcasted_iota(jnp.int32, (total_rows, ep_count), 1)
    spread = jnp.where(slot_rows // cap == slot_experts, 1.0, 0.0).astype(bf16)
    slot_of_row = lax.broadcasted_iota(jnp.int32, (total_rows, seq_count), 0) % cap
    hits = jnp.dot(spread, slots, preferred_element_type=f32) == slot_of_row.astype(f32)
    chooser = jnp.where(hits, 1.0, 0.0)
    place_own[...] = chooser.astype(bf16).reshape(n_groups, block_rows, seq_count)
    place_all[group] = place_own[group]
    tokens_own[...] = jnp.where(core == 0, tokens_ref[:, :half], tokens_ref[:, half:])
    tokens_all[group] = tokens_own[...]

    def across(block, source, target, send_sems, recv_sems):
        return remote(
            source,
            target.at[group],
            send_sems.at[block],
            recv_sems.at[group],
            (target_group(block) * size + rank, core),
        )

    def across_arrival(block, source, target, send_sems, recv_sems):
        origin = source_group(block)
        return remote(
            source,
            target.at[origin],
            send_sems.at[block],
            recv_sems.at[origin],
            (origin * size + rank, core),
        )

    def place_args(block):
        return (block, place_own.at[target_group(block)], place_all, place_send_sems, place_recv_sems)

    def comb_args(block):
        return (block, comb_own.at[target_group(block)], comb_all, comb_send_sems, comb_recv_sems)

    def cross_args(block):
        return (block, tokens_own, tokens_all, cross_send_sems, cross_recv_sems)

    def mix_copy(block, index):
        return remote(
            mix_own,
            mix_all.at[group, core],
            mix_send_sems.at[block, index],
            mix_recv_sems.at[group, core],
            (target_group(block) * size + rank, (core, other)[index]),
        )

    def mix_arrival(block, index):
        origin = source_group(block)
        which = (core, other)[index]
        return remote(
            mix_own,
            mix_all.at[origin, which],
            mix_send_sems.at[block, index],
            mix_recv_sems.at[origin, which],
            (origin * size + rank, which),
        )

    def fan_copy(block, step):
        return remote(
            send_buf.at[block, to_rank[step]],
            rows_buf.at[block, rank],
            fan_send_sems.at[block, step],
            fan_recv_sems.at[block, rank],
            (base + to_rank[step], core),
        )

    def fan_arrival(block, step):
        return remote(
            send_buf.at[block, to_rank[step]],
            rows_buf.at[block, from_rank[step]],
            fan_send_sems.at[block, step],
            fan_recv_sems.at[block, from_rank[step]],
            (base + from_rank[step], core),
        )

    def fan_out(block):
        origin = source_group(block)
        rows = jnp.dot(place_all[origin], rows_all[origin], preferred_element_type=f32)
        send_buf[block] = rows.astype(bf16).reshape(size, cap, half)
        rows_buf[block, rank] = send_buf[block, rank]

    def fan_start(block, chosen):
        for step in chosen:
            fan_copy(block, step).start()

    for load in state_loads:
        load.start()
    pl.semaphore_wait(barrier, 2 * (n_groups - 1) + (size - 1) + 1)
    loads[0].start()
    shares[0].start()
    each(1, n_groups, lambda block: across(*cross_args(block)).start())
    each(1, n_groups, lambda block: across(*place_args(block)).start())

    for load in small[2:5]:
        load.wait()
    tokens = tokens_ref[...].astype(f32)
    factor = lax.rsqrt(jnp.mean(tokens * tokens, axis=1, keepdims=True) + 1e-06)
    normed = (tokens * factor * norm_mix_ref[...].reshape(1, width).astype(f32)).astype(bf16)
    decay_low = jnp.tanh(
        lax.dot_general(normed, decay_down_ref[...], rows_dims, preferred_element_type=f32)
    ).astype(bf16)
    iclr_low = lax.dot_general(
        normed, iclr_down_ref[...], rows_dims, preferred_element_type=f32
    ).astype(bf16)
    for load in small[5:]:
        load.wait()
    decay_in = decay_base_ref[...].reshape(1, channels) + jnp.dot(
        decay_low, decay_up_ref[...], preferred_element_type=f32
    )
    decays = jnp.exp(-jnp.exp(jnp.float32(-0.5)) * jax.nn.sigmoid(decay_in))
    rate = jax.nn.sigmoid(
        iclr_base_ref[...].reshape(1, channels)
        + jnp.dot(iclr_low, iclr_up_ref[...], preferred_element_type=f32)
    )

    def project(index):
        weight_loads[index].wait()
        rows = jnp.dot(normed, weights[index], preferred_element_type=f32)
        return rows.astype(bf16).astype(f32)

    key = project(0)
    scaled = key * key_scale_ref[...].reshape(1, channels).astype(f32)
    key_mod = key * (1.0 + (rate - 1.0) * key_mix_ref[...].reshape(1, channels).astype(f32))
    spans = [slice(head * head_size, (head + 1) * head_size) for head in range(heads)]
    units = []
    for span in spans:
        part = scaled[:, span]
        units.append(part * lax.rsqrt(jnp.sum(part * part, axis=1, keepdims=True) + 1e-06))
    recept = project(1)
    readers, writers, gains = [], [], []
    for head, span in enumerate(spans):
        unit, query = units[head], recept[:, span]
        drop = unit * rate[:, span]
        shift = jnp.sum(drop * query, axis=1, keepdims=True)
        gains.append(jnp.sum(key_mod[:, span] * query, axis=1, keepdims=True))
        reader = decays[:, span] * query - unit * shift
        readers.append(jnp.concatenate([unit, reader], axis=0).astype(bf16))
        writers.append(jnp.concatenate([-drop, key_mod[:, span]], axis=0).astype(bf16))
    value = project(2)
    value_t = jnp.concatenate([value, value], axis=0).T
    for load in loads[1:]:
        load.start()

    def make_rows(origin):
        mixer_out = jnp.zeros((seq_count, half), f32)
        for index in range(2):
            mixer_out += jnp.dot(
                mix_all[origin, index], w_cols[index], preferred_element_type=f32
            )
        mid = tokens_all[origin].astype(f32) + mixer_out.astype(bf16).astype(f32)
        rows_all[origin] = mid.astype(bf16)

    def relay_rows(block):
        across_arrival(*cross_args(block)).wait_recv()
        across_arrival(*place_args(block)).wait_recv()
        for index in range(2):
            mix_arrival(block, index).wait_recv()
        make_rows(source_group(block))
        fan_out(block)
        fan_start(block, steps)

    lanes = lax.broadcasted_iota(jnp.int32, (per_chunk, head_size, 2 * seq_count), 2)
    seqs = lax.broadcasted_iota(jnp.int32, (per_chunk, head_size, 2 * seq_count), 0)
    first = lanes < seq_count
    owner = jnp.where(first, lanes, lanes - seq_count)
    totals = [jnp.zeros((head_size, 2 * seq_count), f32) for _ in range(heads)]
    for index in range(n_chunks):
        rows = slice(index * per_chunk, (index + 1) * per_chunk)
        here = owner == seqs + index * per_chunk
        state_loads[index].wait()
        for head, span in enumerate(spans):
            flat = state_buf[rows, head].reshape(per_chunk * head_size, head_size).astype(bf16)
            read = lax.dot_general(flat, readers[head], rows_dims, preferred_element_type=f32)
            read = read.reshape(per_chunk, head_size, 2 * seq_count)
            totals[head] += jnp.sum(jnp.where(here, read, 0.0), axis=0)
            terms = jnp.where(here, jnp.where(first, read, value_t[span, :][None]), 0.0)
            terms_buf[head, rows] = terms.astype(bf16)
    total = jnp.concatenate(totals, axis=0).T[seq_count:]
    mixed = [total[:, span] + value[:, span] * gains[head] for head, span in enumerate(spans)]
    mixed = jnp.concatenate(mixed, axis=1).astype(bf16)
    for head, span in enumerate(spans):
        decay_buf[head] = decays[:, span]
        writer_buf[head] = writers[head]

    def update_state():
        for index in range(n_chunks):
            rows = slice(index * per_chunk, (index + 1) * per_chunk)
            for head in range(heads):
                terms = terms_buf[head, rows].reshape(per_chunk * head_size, 2 * seq_count)
                change = jnp.dot(terms, writer_buf[head], preferred_element_type=f32)
                state_out_ref[rows, head] = state_buf[rows, head] * decay_buf[head, rows][
                    :, None, :
                ] + change.reshape(per_chunk, head_size, head_size)

    mix_own[...] = mixed

    def send_mixed(block):
        for index in range(2):
            mix_copy(block, index).start()

    each(1, n_groups, send_mixed)
    mix_copy(0, 1).start()
    mix_all[group, core] = mix_own[...]
    loads[0].wait()
    shares[0].wait_recv()
    mix_arrival(0, 1).wait_recv()
    make_rows(group)
    fan_out(0)
    fan_start(0, steps)

    norm_here = jnp.where(core == 0, norm_ref[:half].reshape(1, half), norm_ref[half:].reshape(1, half))
    norm_here = norm_here.astype(f32)
    mid = rows_all[group].astype(f32)
    squares = jnp.sum(mid * mid, axis=1, keepdims=True)
    normed = (mid * norm_here).astype(bf16)
    for router, row in ((router_expert_ref, 0), (router_group_ref, ep_count)):
        columns = jnp.where(core == 0, router[:, :half], router[:, half:])
        logit_own[row : row + router.shape[0], :] = lax.dot_general(
            columns, normed, rows_dims, preferred_element_type=f32
        )
    last = ep_count + n_groups
    logit_own[last : last + 1, :] = jnp.broadcast_to(squares, (seq_count, 128)).T[:1]
    logit_copy = remote(logit_own, logit_recv, logit_sems.at[0], logit_sems.at[1], partner)
    logit_copy.start()
    each(1, n_groups, relay_rows)
    for share in shares[1:]:
        share.start()
    update_state()
    logit_copy.wait_recv()
    logits = logit_own[...] + logit_recv[...]
    logits = logits * lax.rsqrt(logits[last : last + 1] / width + 1e-06)
    expert_logit = logits[:ep_count]
    group_logit = logits[ep_count:last]
    group_prob = jax.nn.sigmoid(jnp.sum(group_logit * group_hit, axis=0, keepdims=True))
    scores = jax.nn.sigmoid(expert_logit) * uses
    route_weights = group_prob * scores / jnp.sum(scores, axis=0, keepdims=True)
    combine = jnp.dot(spread, route_weights.astype(bf16), preferred_element_type=f32) * chooser
    combine = combine.T.astype(bf16)
    for index in range(n_groups):
        comb_own[index] = combine[:, index * block_rows : (index + 1) * block_rows]
    comb_all[group] = comb_own[group]
    each(1, n_groups, lambda block: across(*comb_args(block)).start())

    for load in loads[1:]:
        load.wait()
    for share in shares[1:]:
        share.wait_recv()
    def sums_copy(block):
        return remote(
            sums_own.at[block],
            sums_recv.at[block],
            sums_send_sems.at[block],
            sums_recv_sems.at[block],
            partner,
        )

    def first_products(block):
        for step in reversed(steps):
            fan_arrival(block, step).wait_recv()
        rows = rows_buf[block].reshape(block_rows, half).astype(f32)
        squares = jnp.sum(rows * rows, axis=1, keepdims=True)
        rows = (rows * norm_here).astype(bf16)
        for index in range(2):
            sums_own[block, :, index * hidden_width : (index + 1) * hidden_width] = jnp.dot(
                rows, first_ref[index], preferred_element_type=f32
            )
        tail = sums_own.shape[2] - 2 * hidden_width
        sums_own[block, :, 2 * hidden_width :] = jnp.broadcast_to(squares, (block_rows, tail))
        sums_copy(block).start()

    def back_copy(block, step, piece):
        return remote(
            result_buf.at[piece, block, to_rank[step]],
            back_buf.at[piece, block, rank],
            back_send_sems.at[piece, block, step],
            back_recv_sems.at[piece, block, rank],
            (base + to_rank[step], core),
        )

    def back_arrival(block, step, piece):
        return remote(
            result_buf.at[piece, block, to_rank[step]],
            back_buf.at[piece, block, from_rank[step]],
            back_send_sems.at[piece, block, step],
            back_recv_sems.at[piece, block, from_rank[step]],
            (base + from_rank[step], core),
        )

    def second_product(block):
        sums_copy(block).wait_recv()
        sums = sums_own[block] + sums_recv[block]
        factor = lax.rsqrt(sums[:, 2 * hidden_width : 2 * hidden_width + 1] / width + 1e-06)
        gate_part = sums[:, :hidden_width] * factor
        up_part = sums[:, hidden_width : 2 * hidden_width] * factor
        hidden = (gate_part / (1.0 + jnp.exp(-gate_part)) * up_part).astype(bf16)
        for piece in range(2):
            result = jnp.dot(hidden, down_ref[:, pieces[piece]], preferred_element_type=f32)
            result_buf[piece, block] = result.astype(bf16).reshape(size, cap, half // 2)
            for step in steps:
                back_copy(block, step, piece).start()
            back_buf[piece, block, rank] = result_buf[piece, block, rank]

    first_products(0)
    second_product(0)
    each(1, n_groups, first_products)
    each(1, n_groups, second_product)

    def gather(block, piece):
        for step in reversed(steps):
            back_arrival(block, step, piece).wait_recv()
        back = back_buf[piece, block].reshape(block_rows, half // 2)
        return jnp.dot(comb_all[source_group(block)], back, preferred_element_type=f32)

    def sum_copy(block, piece):
        origin = source_group(block)
        return remote(
            total_send.at[piece, block],
            total_recv.at[piece, group],
            total_send_sems.at[piece, block],
            total_recv_sems.at[piece, group],
            (origin * size + rank, core),
        )

    def sum_arrival(block, piece):
        origin = source_group(block)
        return remote(
            total_send.at[piece, block],
            total_recv.at[piece, origin],
            total_send_sems.at[piece, block],
            total_recv_sems.at[piece, origin],
            (origin * size + rank, core),
        )

    def return_sum(block):
        across_arrival(*comb_args(block)).wait_recv()
        for piece in range(2):
            total_send[piece, block] = gather(block, piece).astype(bf16)
            sum_copy(block, piece).start()

    each(1, n_groups, return_sum)
    for piece, columns in enumerate(pieces):
        final_buf[:, columns] = rows_all[group, :, columns].astype(f32) + gather(0, piece)

    def add_sum(block):
        for piece, columns in enumerate(pieces):
            sum_arrival(block, piece).wait_recv()
            final_buf[:, columns] += total_recv[piece, source_group(block)].astype(f32)

    each(1, n_groups, add_sum)
    out_ref[...] = final_buf[...].astype(bf16)

    def finish_block(block):
        for step in steps:
            fan_copy(block, step).wait_send()
            for piece in range(2):
                back_copy(block, step, piece).wait_send()
        sums_copy(block).wait_send()

    each(0, n_groups, finish_block)

    def finish_cross(block):
        across(*place_args(block)).wait_send()
        across(*cross_args(block)).wait_send()
        for index in range(2):
            mix_copy(block, index).wait_send()
        across(*comb_args(block)).wait_send()
        for piece in range(2):
            sum_copy(block, piece).wait_send()

    each(1, n_groups, finish_cross)
    for share in shares:
        share.wait_send()
    mix_copy(0, 1).wait_send()
    logit_copy.wait_send()


def store_kernel(out_vmem, state_vmem, out_hbm, state_hbm, sems):
    n_chunks = sems.shape[0] - 1
    per_chunk = state_hbm.shape[0] // n_chunks
    copies = [pltpu.make_async_copy(out_vmem, out_hbm, sems.at[n_chunks])]
    for index in range(n_chunks):
        span = pl.ds(index * per_chunk, per_chunk)
        copies.append(
            pltpu.make_async_copy(state_vmem.at[span], state_hbm.at[span], sems.at[index])
        )
    for copy in copies:
        copy.start()
    for copy in copies:
        copy.wait()


def shards(
    tokens_in,
    state_in,
    norm_mix,
    w_recept,
    w_key,
    w_value,
    decay_down,
    decay_up,
    decay_base,
    iclr_down,
    iclr_up,
    iclr_base,
    key_scale,
    key_mix,
    w_out,
    norm_moe,
    router_group,
    router_expert,
    routes,
    expert_gate,
    expert_up,
    expert_down,
):
    f32 = jnp.float32
    bf16 = jnp.bfloat16
    seq_count, width_model = tokens_in.shape
    heads_here, head_size = state_in.shape[1], state_in.shape[3]
    channels = heads_here * head_size
    tp_count = lax.axis_size("tp")
    ep_count = lax.axis_size("ep")
    dma = pltpu.SemaphoreType.DMA
    vmem = pl.BlockSpec(memory_space=pltpu.VMEM)
    anywhere = pl.BlockSpec(memory_space=pl.ANY)
    n_chunks = 2 if seq_count % 2 == 0 else 1
    top_count = routes.shape[1]
    half_width = width_model // tp_count
    limit = max(2, 2 * seq_count * top_count // ep_count)
    cap = -(-limit // 16) * 16
    n_groups = router_group.shape[1]
    size = ep_count // n_groups
    block_rows = size * cap
    hidden_width = expert_gate.shape[2]
    block_bytes = ep_count * cap * width_model
    vmem_limit = min(58 * 1024 * 1024, 24 * 1024 * 1024 + 10 * block_bytes)
    vmem_of = pltpu.VMEM
    small = (
        tokens_in, routes.T, norm_mix, decay_down.T, iclr_down.T, decay_up, decay_base,
        iclr_up, iclr_base, key_scale, key_mix, norm_moe, router_group.T, router_expert.T,
    )
    large = (
        w_recept, w_key, w_value, state_in, w_out, expert_gate, expert_up, expert_down,
    )
    operands = small + large
    layer = pl.pallas_call(
        functools.partial(layer_kernel, ep_count),
        out_shape=(
            jax.ShapeDtypeStruct((seq_count, half_width), bf16),
            jax.ShapeDtypeStruct(state_in.shape, f32),
        ),
        in_specs=[anywhere] * len(operands),
        out_specs=(vmem, vmem),
        scratch_shapes=[vmem_of(operand.shape, operand.dtype) for operand in small]
        + [
            vmem_of((3, width_model, channels), bf16),
            vmem_of(state_in.shape, f32),
            vmem_of((heads_here, seq_count, head_size, 2 * seq_count), bf16),
            vmem_of((heads_here, seq_count, head_size), f32),
            vmem_of((heads_here, 2 * seq_count, head_size), bf16),
            vmem_of((tp_count, channels, half_width), bf16),
            vmem_of((2, half_width, tp_count * hidden_width), bf16),
            vmem_of((tp_count * hidden_width, half_width), bf16),
            vmem_of((seq_count, half_width), f32),
            vmem_of((ep_count + n_groups + 1, seq_count), f32),
            vmem_of((ep_count + n_groups + 1, seq_count), f32),
            vmem_of((n_groups, block_rows, seq_count), bf16),
            vmem_of((n_groups, block_rows, seq_count), bf16),
            vmem_of((n_groups, seq_count, block_rows), bf16),
            vmem_of((n_groups, seq_count, block_rows), bf16),
            vmem_of((seq_count, half_width), bf16),
            vmem_of((n_groups, seq_count, half_width), bf16),
            vmem_of((seq_count, channels), bf16),
            vmem_of((n_groups, tp_count, seq_count, channels), bf16),
            vmem_of((n_groups, seq_count, half_width), bf16),
            vmem_of((n_groups, size, cap, half_width), bf16),
            vmem_of((n_groups, size, cap, half_width), bf16),
            vmem_of((n_groups, block_rows, 2 * tp_count * hidden_width + 128), f32),
            vmem_of((n_groups, block_rows, 2 * tp_count * hidden_width + 128), f32),
            vmem_of((2, n_groups, size, cap, half_width // 2), bf16),
            vmem_of((2, n_groups, size, cap, half_width // 2), bf16),
            vmem_of((2, n_groups, seq_count, half_width // 2), bf16),
            vmem_of((2, n_groups, seq_count, half_width // 2), bf16),
            dma((len(small),)),
            dma((3,)),
            dma((n_chunks,)),
            dma((4,)),
            dma((4,)),
            dma((4,)),
            dma((2,)),
            dma((n_groups,)),
            dma((n_groups,)),
            dma((n_groups,)),
            dma((n_groups,)),
            dma((n_groups,)),
            dma((n_groups,)),
            dma((n_groups, tp_count)),
            dma((n_groups, tp_count)),
            dma((n_groups, size)),
            dma((n_groups, size)),
            dma((n_groups,)),
            dma((n_groups,)),
            dma((2, n_groups, size)),
            dma((2, n_groups, size)),
            dma((2, n_groups)),
            dma((2, n_groups)),
        ],
        compiler_params=pltpu.CompilerParams(
            collective_id=0, has_side_effects=True, vmem_limit_bytes=vmem_limit
        ),
    )
    layer_out, state_out = layer(
        *(pltpu.with_memory_space_constraint(operand, pltpu.HBM) for operand in operands)
    )
    pieces = 4 if seq_count % 4 == 0 else 1
    return pl.pallas_call(
        store_kernel,
        out_shape=(
            jax.ShapeDtypeStruct(layer_out.shape, bf16),
            jax.ShapeDtypeStruct(state_in.shape, f32),
        ),
        in_specs=[vmem, vmem],
        out_specs=(anywhere, anywhere),
        scratch_shapes=[dma((pieces + 1,))],
        compiler_params=pltpu.CompilerParams(vmem_limit_bytes=8 * 1024 * 1024),
    )(layer_out, state_out)


def solution(mesh):
    in_specs = (
        P("ep", None),
        P("ep", "tp", None, None),
        P(),
        P(None, "tp"),
        P(None, "tp"),
        P(None, "tp"),
        P(),
        P(None, "tp"),
        P("tp"),
        P(),
        P(None, "tp"),
        P("tp"),
        P("tp"),
        P("tp"),
        P("tp", None),
        P(),
        P(),
        P(),
        P("ep", None),
        P("ep", None, "tp"),
        P("ep", None, "tp"),
        P("ep", "tp", None),
    )
    out_specs = (P("ep", "tp"), P("ep", "tp", None, None))
    return jax.shard_map(shards, mesh=mesh, in_specs=in_specs, out_specs=out_specs, check_vma=False)
```

```python
import functools

import jax
import jax.numpy as jnp
from jax import lax
from jax.experimental import pallas as pl
from jax.experimental.pallas import tpu as pltpu
from jax.sharding import PartitionSpec as P


def layer_kernel(
    ep_count,
    tokens_hbm,
    routes_hbm,
    norm_mix_hbm,
    decay_down_hbm,
    iclr_down_hbm,
    decay_up_hbm,
    decay_base_hbm,
    iclr_up_hbm,
    iclr_base_hbm,
    key_scale_hbm,
    key_mix_hbm,
    norm_moe_hbm,
    router_group_hbm,
    router_expert_hbm,
    w_recept_hbm,
    w_key_hbm,
    w_value_hbm,
    state_hbm,
    w_out_hbm,
    gate_hbm,
    up_hbm,
    down_hbm,
    out_ref,
    state_out_ref,
    tokens_ref,
    routes_ref,
    norm_mix_ref,
    decay_down_ref,
    iclr_down_ref,
    decay_up_ref,
    decay_base_ref,
    iclr_up_ref,
    iclr_base_ref,
    key_scale_ref,
    key_mix_ref,
    norm_ref,
    router_group_ref,
    router_expert_ref,
    weights,
    state_buf,
    terms_buf,
    decay_buf,
    writer_buf,
    w_cols,
    first_ref,
    down_ref,
    final_buf,
    logit_own,
    logit_recv,
    place_own,
    place_all,
    comb_own,
    comb_all,
    tokens_own,
    tokens_all,
    mix_own,
    mix_all,
    rows_all,
    send_buf,
    rows_buf,
    sums_own,
    sums_recv,
    result_buf,
    back_buf,
    total_send,
    total_recv,
    small_sems,
    weight_sems,
    in_sems,
    load_sems,
    share_send_sems,
    share_recv_sems,
    logit_sems,
    place_send_sems,
    place_recv_sems,
    comb_send_sems,
    comb_recv_sems,
    cross_send_sems,
    cross_recv_sems,
    mix_send_sems,
    mix_recv_sems,
    fan_send_sems,
    fan_recv_sems,
    sums_send_sems,
    sums_recv_sems,
    back_send_sems,
    back_recv_sems,
    total_send_sems,
    total_recv_sems,
):
    f32 = jnp.float32
    bf16 = jnp.bfloat16
    me = lax.axis_index("ep")
    core = lax.axis_index("tp")
    other = 1 - core
    seq_count, width = tokens_ref.shape
    half = width // 2
    heads, head_size = state_hbm.shape[1], state_hbm.shape[3]
    channels = heads * head_size
    rows_dims = (((1,), (1,)), ((), ()))
    cap = send_buf.shape[2]
    total_rows = ep_count * cap
    mesh_ids = pl.DeviceIdType.MESH
    n_groups = router_group_ref.shape[0]
    size = ep_count // n_groups
    group = me // size
    rank = me % size
    base = group * size
    block_rows = size * cap
    hidden_part = gate_hbm.shape[2]
    hidden_width = 2 * hidden_part
    power = size & (size - 1) == 0
    steps = sorted(range(1, size), key=lambda step: -bin(step).count("1"))
    near = [step for step in steps if 2 * step < size]
    far = [step for step in steps if 2 * step >= size]

    def flip(step):
        moved = rank * 0
        bit = 1
        while bit < size:
            value = rank // bit % 2
            moved = moved + bit * ((1 - value) if step & bit else value)
            bit *= 2
        return moved

    to_rank = {s: flip(s) if power else (rank + s) % size for s in steps}
    from_rank = {s: flip(s) if power else (rank + size - s) % size for s in steps}

    def each(low, high, visit):
        if high - low <= 2:
            for index in range(low, high):
                visit(index)
        else:
            lax.fori_loop(low, high, lambda index, carry: (visit(index), carry)[1], 0)

    def source_group(block):
        return (group + n_groups - block) % n_groups

    def target_group(block):
        return (group + block) % n_groups

    def remote(source, target, send_sem, recv_sem, device):
        return pltpu.make_async_remote_copy(
            src_ref=source,
            dst_ref=target,
            send_sem=send_sem,
            recv_sem=recv_sem,
            device_id=device,
            device_id_type=mesh_ids,
        )

    partner = (me, other)
    pieces = (slice(0, half // 2), slice(half // 2, half))
    barrier = pltpu.get_barrier_semaphore()

    def greet(device):
        pl.semaphore_signal(barrier, inc=1, device_id=device, device_id_type=mesh_ids)

    for which in (core, other):
        each(1, n_groups, lambda block: greet((target_group(block) * size + rank, which)))
    for step in steps:
        greet((base + to_rank[step], core))
    greet(partner)

    small = [
        pltpu.make_async_copy(source, target, small_sems.at[index])
        for index, (source, target) in enumerate(
            (
                (tokens_hbm, tokens_ref),
                (routes_hbm, routes_ref),
                (norm_mix_hbm, norm_mix_ref),
                (decay_down_hbm, decay_down_ref),
                (iclr_down_hbm, iclr_down_ref),
                (decay_up_hbm, decay_up_ref),
                (decay_base_hbm, decay_base_ref),
                (iclr_up_hbm, iclr_up_ref),
                (iclr_base_hbm, iclr_base_ref),
                (key_scale_hbm, key_scale_ref),
                (key_mix_hbm, key_mix_ref),
                (norm_moe_hbm, norm_ref),
                (router_group_hbm, router_group_ref),
                (router_expert_hbm, router_expert_ref),
            )
        )
    ]
    for load in small:
        load.start()
    weight_loads = [
        pltpu.make_async_copy(source, weights.at[index], weight_sems.at[index])
        for index, source in enumerate((w_key_hbm, w_recept_hbm, w_value_hbm))
    ]
    for load in weight_loads:
        load.start()
    n_chunks = in_sems.shape[0]
    per_chunk = seq_count // n_chunks
    state_loads = []
    for index in range(n_chunks):
        span = pl.ds(index * per_chunk, per_chunk)
        state_loads.append(
            pltpu.make_async_copy(state_hbm.at[span], state_buf.at[span], in_sems.at[index])
        )

    def columns_of(which):
        return pl.ds(pl.multiple_of(which * half, half), half)

    hidden_here = pl.ds(pl.multiple_of(core * hidden_part, hidden_part), hidden_part)
    shared = (
        (lambda which: w_out_hbm.at[:, columns_of(which)], w_cols.at[core]),
        (lambda which: gate_hbm.at[0, columns_of(which)], first_ref.at[0, :, hidden_here]),
        (lambda which: up_hbm.at[0, columns_of(which)], first_ref.at[1, :, hidden_here]),
        (lambda which: down_hbm.at[0, :, columns_of(which)], down_ref.at[hidden_here]),
    )
    loads = []
    shares = []
    for index, (source, target) in enumerate(shared):
        loads.append(pltpu.make_async_copy(source(core), target, load_sems.at[index]))
        shares.append(
            remote(
                source(other), target, share_send_sems.at[index], share_recv_sems.at[index], partner
            )
        )
    for load in small[:2]:
        load.wait()

    expert_ids = lax.broadcasted_iota(jnp.int32, (ep_count, seq_count), 0)
    uses = jnp.zeros((ep_count, seq_count), f32)
    for index in range(routes_ref.shape[0]):
        uses += jnp.where(routes_ref[index : index + 1, :] == expert_ids, 1.0, 0.0)
    group_ids = lax.broadcasted_iota(jnp.int32, (n_groups, seq_count), 0)
    group_hit = jnp.where(routes_ref[0:1, :] // size == group_ids, 1.0, 0.0)
    row_ids = lax.broadcasted_iota(jnp.int32, (seq_count, seq_count), 0)
    column_ids = lax.broadcasted_iota(jnp.int32, (seq_count, seq_count), 1)
    earlier = jnp.where(row_ids < column_ids, 1.0, 0.0).astype(bf16)
    position = jnp.dot(uses.astype(bf16), earlier, preferred_element_type=f32)
    slots = jnp.where(uses > 0.5, position, -1.0).astype(bf16)
    slot_rows = lax.broadcasted_iota(jnp.int32, (total_rows, ep_count), 0)
    slot_experts = lax.broadcasted_iota(jnp.int32, (total_rows, ep_count), 1)
    spread = jnp.where(slot_rows // cap == slot_experts, 1.0, 0.0).astype(bf16)
    slot_of_row = lax.broadcasted_iota(jnp.int32, (total_rows, seq_count), 0) % cap
    hits = jnp.dot(spread, slots, preferred_element_type=f32) == slot_of_row.astype(f32)
    chooser = jnp.where(hits, 1.0, 0.0)
    place_own[...] = chooser.astype(bf16).reshape(n_groups, block_rows, seq_count)
    place_all[group] = place_own[group]
    tokens_own[...] = jnp.where(core == 0, tokens_ref[:, :half], tokens_ref[:, half:])
    tokens_all[group] = tokens_own[...]

    def across(block, source, target, send_sems, recv_sems):
        return remote(
            source,
            target.at[group],
            send_sems.at[block],
            recv_sems.at[group],
            (target_group(block) * size + rank, core),
        )

    def across_arrival(block, source, target, send_sems, recv_sems):
        origin = source_group(block)
        return remote(
            source,
            target.at[origin],
            send_sems.at[block],
            recv_sems.at[origin],
            (origin * size + rank, core),
        )

    def place_args(block):
        return (block, place_own.at[target_group(block)], place_all, place_send_sems, place_recv_sems)

    def comb_args(block):
        return (block, comb_own.at[target_group(block)], comb_all, comb_send_sems, comb_recv_sems)

    def cross_args(block):
        return (block, tokens_own, tokens_all, cross_send_sems, cross_recv_sems)

    def mix_copy(block, index):
        return remote(
            mix_own,
            mix_all.at[group, core],
            mix_send_sems.at[block, index],
            mix_recv_sems.at[group, core],
            (target_group(block) * size + rank, (core, other)[index]),
        )

    def mix_arrival(block, index):
        origin = source_group(block)
        which = (core, other)[index]
        return remote(
            mix_own,
            mix_all.at[origin, which],
            mix_send_sems.at[block, index],
            mix_recv_sems.at[origin, which],
            (origin * size + rank, which),
        )

    def fan_copy(block, step):
        return remote(
            send_buf.at[block, to_rank[step]],
            rows_buf.at[block, rank],
            fan_send_sems.at[block, step],
            fan_recv_sems.at[block, rank],
            (base + to_rank[step], core),
        )

    def fan_arrival(block, step):
        return remote(
            send_buf.at[block, to_rank[step]],
            rows_buf.at[block, from_rank[step]],
            fan_send_sems.at[block, step],
            fan_recv_sems.at[block, from_rank[step]],
            (base + from_rank[step], core),
        )

    def fan_out(block):
        origin = source_group(block)
        rows = jnp.dot(place_all[origin], rows_all[origin], preferred_element_type=f32)
        send_buf[block] = rows.astype(bf16).reshape(size, cap, half)
        rows_buf[block, rank] = send_buf[block, rank]

    def fan_start(block, chosen):
        for step in chosen:
            fan_copy(block, step).start()

    for load in state_loads:
        load.start()
    pl.semaphore_wait(barrier, 2 * (n_groups - 1) + (size - 1) + 1)
    loads[0].start()
    shares[0].start()
    each(1, n_groups, lambda block: across(*cross_args(block)).start())
    each(1, n_groups, lambda block: across(*place_args(block)).start())

    for load in small[2:5]:
        load.wait()
    tokens = tokens_ref[...].astype(f32)
    factor = lax.rsqrt(jnp.mean(tokens * tokens, axis=1, keepdims=True) + 1e-06)
    normed = (tokens * factor * norm_mix_ref[...].reshape(1, width).astype(f32)).astype(bf16)
    decay_low = jnp.tanh(
        lax.dot_general(normed, decay_down_ref[...], rows_dims, preferred_element_type=f32)
    ).astype(bf16)
    iclr_low = lax.dot_general(
        normed, iclr_down_ref[...], rows_dims, preferred_element_type=f32
    ).astype(bf16)
    for load in small[5:]:
        load.wait()
    decay_in = decay_base_ref[...].reshape(1, channels) + jnp.dot(
        decay_low, decay_up_ref[...], preferred_element_type=f32
    )
    decays = jnp.exp(-jnp.exp(jnp.float32(-0.5)) * jax.nn.sigmoid(decay_in))
    rate = jax.nn.sigmoid(
        iclr_base_ref[...].reshape(1, channels)
        + jnp.dot(iclr_low, iclr_up_ref[...], preferred_element_type=f32)
    )

    def project(index):
        weight_loads[index].wait()
        rows = jnp.dot(normed, weights[index], preferred_element_type=f32)
        return rows.astype(bf16).astype(f32)

    key = project(0)
    scaled = key * key_scale_ref[...].reshape(1, channels).astype(f32)
    key_mod = key * (1.0 + (rate - 1.0) * key_mix_ref[...].reshape(1, channels).astype(f32))
    spans = [slice(head * head_size, (head + 1) * head_size) for head in range(heads)]
    units = []
    for span in spans:
        part = scaled[:, span]
        units.append(part * lax.rsqrt(jnp.sum(part * part, axis=1, keepdims=True) + 1e-06))
    recept = project(1)
    readers, writers, gains = [], [], []
    for head, span in enumerate(spans):
        unit, query = units[head], recept[:, span]
        drop = unit * rate[:, span]
        shift = jnp.sum(drop * query, axis=1, keepdims=True)
        gains.append(jnp.sum(key_mod[:, span] * query, axis=1, keepdims=True))
        reader = decays[:, span] * query - unit * shift
        readers.append(jnp.concatenate([unit, reader], axis=0).astype(bf16))
        writers.append(jnp.concatenate([-drop, key_mod[:, span]], axis=0).astype(bf16))
    value = project(2)
    value_t = jnp.concatenate([value, value], axis=0).T
    for load in loads[1:]:
        load.start()

    def make_rows(origin):
        mixer_out = jnp.zeros((seq_count, half), f32)
        for index in range(2):
            mixer_out += jnp.dot(
                mix_all[origin, index], w_cols[index], preferred_element_type=f32
            )
        mid = tokens_all[origin].astype(f32) + mixer_out.astype(bf16).astype(f32)
        rows_all[origin] = mid.astype(bf16)

    def relay_rows(block):
        across_arrival(*cross_args(block)).wait_recv()
        across_arrival(*place_args(block)).wait_recv()
        for index in range(2):
            mix_arrival(block, index).wait_recv()
        make_rows(source_group(block))
        fan_out(block)
        fan_start(block, steps)

    lanes = lax.broadcasted_iota(jnp.int32, (per_chunk, head_size, 2 * seq_count), 2)
    seqs = lax.broadcasted_iota(jnp.int32, (per_chunk, head_size, 2 * seq_count), 0)
    first = lanes < seq_count
    owner = jnp.where(first, lanes, lanes - seq_count)
    totals = [jnp.zeros((head_size, 2 * seq_count), f32) for _ in range(heads)]
    for index in range(n_chunks):
        rows = slice(index * per_chunk, (index + 1) * per_chunk)
        here = owner == seqs + index * per_chunk
        state_loads[index].wait()
        for head, span in enumerate(spans):
            flat = state_buf[rows, head].reshape(per_chunk * head_size, head_size).astype(bf16)
            read = lax.dot_general(flat, readers[head], rows_dims, preferred_element_type=f32)
            read = read.reshape(per_chunk, head_size, 2 * seq_count)
            totals[head] += jnp.sum(jnp.where(here, read, 0.0), axis=0)
            terms = jnp.where(here, jnp.where(first, read, value_t[span, :][None]), 0.0)
            terms_buf[head, rows] = terms.astype(bf16)
    total = jnp.concatenate(totals, axis=0).T[seq_count:]
    mixed = [total[:, span] + value[:, span] * gains[head] for head, span in enumerate(spans)]
    mixed = jnp.concatenate(mixed, axis=1).astype(bf16)
    for head, span in enumerate(spans):
        decay_buf[head] = decays[:, span]
        writer_buf[head] = writers[head]

    def update_state():
        for index in range(n_chunks):
            rows = slice(index * per_chunk, (index + 1) * per_chunk)
            for head in range(heads):
                terms = terms_buf[head, rows].reshape(per_chunk * head_size, 2 * seq_count)
                change = jnp.dot(terms, writer_buf[head], preferred_element_type=f32)
                state_out_ref[rows, head] = state_buf[rows, head] * decay_buf[head, rows][
                    :, None, :
                ] + change.reshape(per_chunk, head_size, head_size)

    mix_own[...] = mixed

    def send_mixed(block):
        for index in range(2):
            mix_copy(block, index).start()

    each(1, n_groups, send_mixed)
    mix_copy(0, 1).start()
    mix_all[group, core] = mix_own[...]
    loads[0].wait()
    shares[0].wait_recv()
    mixer_out = jnp.dot(mixed, w_cols[core], preferred_element_type=f32)
    mix_arrival(0, 1).wait_recv()
    mixer_out += jnp.dot(mix_all[group, other], w_cols[other], preferred_element_type=f32)
    mid = tokens_all[group].astype(f32) + mixer_out.astype(bf16).astype(f32)
    rows_all[group] = mid.astype(bf16)
    fan_out(0)
    fan_start(0, steps)

    norm_here = jnp.where(core == 0, norm_ref[:half].reshape(1, half), norm_ref[half:].reshape(1, half))
    norm_here = norm_here.astype(f32)
    mid = rows_all[group].astype(f32)
    squares = jnp.sum(mid * mid, axis=1, keepdims=True)
    normed = (mid * norm_here).astype(bf16)
    for router, row in ((router_expert_ref, 0), (router_group_ref, ep_count)):
        columns = jnp.where(core == 0, router[:, :half], router[:, half:])
        logit_own[row : row + router.shape[0], :] = lax.dot_general(
            columns, normed, rows_dims, preferred_element_type=f32
        )
    last = ep_count + n_groups
    logit_own[last : last + 1, :] = jnp.broadcast_to(squares, (seq_count, 128)).T[:1]
    logit_copy = remote(logit_own, logit_recv, logit_sems.at[0], logit_sems.at[1], partner)
    logit_copy.start()
    each(1, n_groups, relay_rows)
    for share in shares[1:]:
        share.start()
    update_state()
    logit_copy.wait_recv()
    logits = logit_own[...] + logit_recv[...]
    logits = logits * lax.rsqrt(logits[last : last + 1] / width + 1e-06)
    expert_logit = logits[:ep_count]
    group_logit = logits[ep_count:last]
    group_prob = jax.nn.sigmoid(jnp.sum(group_logit * group_hit, axis=0, keepdims=True))
    scores = jax.nn.sigmoid(expert_logit) * uses
    route_weights = group_prob * scores / jnp.sum(scores, axis=0, keepdims=True)
    combine = jnp.dot(spread, route_weights.astype(bf16), preferred_element_type=f32) * chooser
    combine = combine.T.astype(bf16)
    for index in range(n_groups):
        comb_own[index] = combine[:, index * block_rows : (index + 1) * block_rows]
    comb_all[group] = comb_own[group]
    each(1, n_groups, lambda block: across(*comb_args(block)).start())

    for load in loads[1:]:
        load.wait()
    for share in shares[1:]:
        share.wait_recv()
    def sums_copy(block):
        return remote(
            sums_own.at[block],
            sums_recv.at[block],
            sums_send_sems.at[block],
            sums_recv_sems.at[block],
            partner,
        )

    def first_products(block):
        for step in reversed(steps):
            fan_arrival(block, step).wait_recv()
        rows = rows_buf[block].reshape(block_rows, half).astype(f32)
        squares = jnp.sum(rows * rows, axis=1, keepdims=True)
        rows = (rows * norm_here).astype(bf16)
        for index in range(2):
            sums_own[block, :, index * hidden_width : (index + 1) * hidden_width] = jnp.dot(
                rows, first_ref[index], preferred_element_type=f32
            )
        tail = sums_own.shape[2] - 2 * hidden_width
        sums_own[block, :, 2 * hidden_width :] = jnp.broadcast_to(squares, (block_rows, tail))
        sums_copy(block).start()

    def back_copy(block, step, piece):
        return remote(
            result_buf.at[piece, block, to_rank[step]],
            back_buf.at[piece, block, rank],
            back_send_sems.at[piece, block, step],
            back_recv_sems.at[piece, block, rank],
            (base + to_rank[step], core),
        )

    def back_arrival(block, step, piece):
        return remote(
            result_buf.at[piece, block, to_rank[step]],
            back_buf.at[piece, block, from_rank[step]],
            back_send_sems.at[piece, block, step],
            back_recv_sems.at[piece, block, from_rank[step]],
            (base + from_rank[step], core),
        )

    def second_product(block):
        sums_copy(block).wait_recv()
        sums = sums_own[block] + sums_recv[block]
        factor = lax.rsqrt(sums[:, 2 * hidden_width : 2 * hidden_width + 1] / width + 1e-06)
        gate_part = sums[:, :hidden_width] * factor
        up_part = sums[:, hidden_width : 2 * hidden_width] * factor
        hidden = (gate_part / (1.0 + jnp.exp(-gate_part)) * up_part).astype(bf16)
        for piece in range(2):
            result = jnp.dot(hidden, down_ref[:, pieces[piece]], preferred_element_type=f32)
            result_buf[piece, block] = result.astype(bf16).reshape(size, cap, half // 2)
            for step in steps:
                back_copy(block, step, piece).start()
            back_buf[piece, block, rank] = result_buf[piece, block, rank]

    first_products(0)
    second_product(0)
    each(1, n_groups, first_products)
    each(1, n_groups, second_product)

    def gather(block, piece):
        for step in reversed(steps):
            back_arrival(block, step, piece).wait_recv()
        back = back_buf[piece, block].reshape(block_rows, half // 2)
        return jnp.dot(comb_all[source_group(block)], back, preferred_element_type=f32)

    def sum_copy(block, piece):
        origin = source_group(block)
        return remote(
            total_send.at[piece, block],
            total_recv.at[piece, group],
            total_send_sems.at[piece, block],
            total_recv_sems.at[piece, group],
            (origin * size + rank, core),
        )

    def sum_arrival(block, piece):
        origin = source_group(block)
        return remote(
            total_send.at[piece, block],
            total_recv.at[piece, origin],
            total_send_sems.at[piece, block],
            total_recv_sems.at[piece, origin],
            (origin * size + rank, core),
        )

    def return_sum(block):
        across_arrival(*comb_args(block)).wait_recv()
        for piece in range(2):
            total_send[piece, block] = gather(block, piece).astype(bf16)
            sum_copy(block, piece).start()

    each(1, n_groups, return_sum)
    for piece, columns in enumerate(pieces):
        final_buf[:, columns] = rows_all[group, :, columns].astype(f32) + gather(0, piece)

    def add_sum(block):
        for piece, columns in enumerate(pieces):
            sum_arrival(block, piece).wait_recv()
            final_buf[:, columns] += total_recv[piece, source_group(block)].astype(f32)

    each(1, n_groups, add_sum)
    out_ref[...] = final_buf[...].astype(bf16)

    def finish_block(block):
        for step in steps:
            fan_copy(block, step).wait_send()
            for piece in range(2):
                back_copy(block, step, piece).wait_send()
        sums_copy(block).wait_send()

    each(0, n_groups, finish_block)

    def finish_cross(block):
        across(*place_args(block)).wait_send()
        across(*cross_args(block)).wait_send()
        for index in range(2):
            mix_copy(block, index).wait_send()
        across(*comb_args(block)).wait_send()
        for piece in range(2):
            sum_copy(block, piece).wait_send()

    each(1, n_groups, finish_cross)
    for share in shares:
        share.wait_send()
    mix_copy(0, 1).wait_send()
    logit_copy.wait_send()


def store_kernel(out_vmem, state_vmem, out_hbm, state_hbm, sems):
    n_chunks = sems.shape[0] - 1
    per_chunk = state_hbm.shape[0] // n_chunks
    copies = [pltpu.make_async_copy(out_vmem, out_hbm, sems.at[n_chunks])]
    for index in range(n_chunks):
        span = pl.ds(index * per_chunk, per_chunk)
        copies.append(
            pltpu.make_async_copy(state_vmem.at[span], state_hbm.at[span], sems.at[index])
        )
    for copy in copies:
        copy.start()
    for copy in copies:
        copy.wait()


def shards(
    tokens_in,
    state_in,
    norm_mix,
    w_recept,
    w_key,
    w_value,
    decay_down,
    decay_up,
    decay_base,
    iclr_down,
    iclr_up,
    iclr_base,
    key_scale,
    key_mix,
    w_out,
    norm_moe,
    router_group,
    router_expert,
    routes,
    expert_gate,
    expert_up,
    expert_down,
):
    f32 = jnp.float32
    bf16 = jnp.bfloat16
    seq_count, width_model = tokens_in.shape
    heads_here, head_size = state_in.shape[1], state_in.shape[3]
    channels = heads_here * head_size
    tp_count = lax.axis_size("tp")
    ep_count = lax.axis_size("ep")
    dma = pltpu.SemaphoreType.DMA
    vmem = pl.BlockSpec(memory_space=pltpu.VMEM)
    anywhere = pl.BlockSpec(memory_space=pl.ANY)
    n_chunks = 2 if seq_count % 2 == 0 else 1
    top_count = routes.shape[1]
    half_width = width_model // tp_count
    limit = max(2, 2 * seq_count * top_count // ep_count)
    cap = -(-limit // 16) * 16
    n_groups = router_group.shape[1]
    size = ep_count // n_groups
    block_rows = size * cap
    hidden_width = expert_gate.shape[2]
    block_bytes = ep_count * cap * width_model
    vmem_limit = min(58 * 1024 * 1024, 24 * 1024 * 1024 + 10 * block_bytes)
    vmem_of = pltpu.VMEM
    small = (
        tokens_in, routes.T, norm_mix, decay_down.T, iclr_down.T, decay_up, decay_base,
        iclr_up, iclr_base, key_scale, key_mix, norm_moe, router_group.T, router_expert.T,
    )
    large = (
        w_recept, w_key, w_value, state_in, w_out, expert_gate, expert_up, expert_down,
    )
    operands = small + large
    layer = pl.pallas_call(
        functools.partial(layer_kernel, ep_count),
        out_shape=(
            jax.ShapeDtypeStruct((seq_count, half_width), bf16),
            jax.ShapeDtypeStruct(state_in.shape, f32),
        ),
        in_specs=[anywhere] * len(operands),
        out_specs=(vmem, vmem),
        scratch_shapes=[vmem_of(operand.shape, operand.dtype) for operand in small]
        + [
            vmem_of((3, width_model, channels), bf16),
            vmem_of(state_in.shape, f32),
            vmem_of((heads_here, seq_count, head_size, 2 * seq_count), bf16),
            vmem_of((heads_here, seq_count, head_size), f32),
            vmem_of((heads_here, 2 * seq_count, head_size), bf16),
            vmem_of((tp_count, channels, half_width), bf16),
            vmem_of((2, half_width, tp_count * hidden_width), bf16),
            vmem_of((tp_count * hidden_width, half_width), bf16),
            vmem_of((seq_count, half_width), f32),
            vmem_of((ep_count + n_groups + 1, seq_count), f32),
            vmem_of((ep_count + n_groups + 1, seq_count), f32),
            vmem_of((n_groups, block_rows, seq_count), bf16),
            vmem_of((n_groups, block_rows, seq_count), bf16),
            vmem_of((n_groups, seq_count, block_rows), bf16),
            vmem_of((n_groups, seq_count, block_rows), bf16),
            vmem_of((seq_count, half_width), bf16),
            vmem_of((n_groups, seq_count, half_width), bf16),
            vmem_of((seq_count, channels), bf16),
            vmem_of((n_groups, tp_count, seq_count, channels), bf16),
            vmem_of((n_groups, seq_count, half_width), bf16),
            vmem_of((n_groups, size, cap, half_width), bf16),
            vmem_of((n_groups, size, cap, half_width), bf16),
            vmem_of((n_groups, block_rows, 2 * tp_count * hidden_width + 128), f32),
            vmem_of((n_groups, block_rows, 2 * tp_count * hidden_width + 128), f32),
            vmem_of((2, n_groups, size, cap, half_width // 2), bf16),
            vmem_of((2, n_groups, size, cap, half_width // 2), bf16),
            vmem_of((2, n_groups, seq_count, half_width // 2), bf16),
            vmem_of((2, n_groups, seq_count, half_width // 2), bf16),
            dma((len(small),)),
            dma((3,)),
            dma((n_chunks,)),
            dma((4,)),
            dma((4,)),
            dma((4,)),
            dma((2,)),
            dma((n_groups,)),
            dma((n_groups,)),
            dma((n_groups,)),
            dma((n_groups,)),
            dma((n_groups,)),
            dma((n_groups,)),
            dma((n_groups, tp_count)),
            dma((n_groups, tp_count)),
            dma((n_groups, size)),
            dma((n_groups, size)),
            dma((n_groups,)),
            dma((n_groups,)),
            dma((2, n_groups, size)),
            dma((2, n_groups, size)),
            dma((2, n_groups)),
            dma((2, n_groups)),
        ],
        compiler_params=pltpu.CompilerParams(
            collective_id=0, has_side_effects=True, vmem_limit_bytes=vmem_limit
        ),
    )
    layer_out, state_out = layer(
        *(pltpu.with_memory_space_constraint(operand, pltpu.HBM) for operand in operands)
    )
    pieces = 4 if seq_count % 4 == 0 else 1
    return pl.pallas_call(
        store_kernel,
        out_shape=(
            jax.ShapeDtypeStruct(layer_out.shape, bf16),
            jax.ShapeDtypeStruct(state_in.shape, f32),
        ),
        in_specs=[vmem, vmem],
        out_specs=(anywhere, anywhere),
        scratch_shapes=[dma((pieces + 1,))],
        compiler_params=pltpu.CompilerParams(vmem_limit_bytes=8 * 1024 * 1024),
    )(layer_out, state_out)


def solution(mesh):
    in_specs = (
        P("ep", None),
        P("ep", "tp", None, None),
        P(),
        P(None, "tp"),
        P(None, "tp"),
        P(None, "tp"),
        P(),
        P(None, "tp"),
        P("tp"),
        P(),
        P(None, "tp"),
        P("tp"),
        P("tp"),
        P("tp"),
        P("tp", None),
        P(),
        P(),
        P(),
        P("ep", None),
        P("ep", None, "tp"),
        P("ep", None, "tp"),
        P("ep", "tp", None),
    )
    out_specs = (P("ep", "tp"), P("ep", "tp", None, None))
    return jax.shard_map(shards, mesh=mesh, in_specs=in_specs, out_specs=out_specs, check_vma=False)
```
